256 devices in a mesh: dp: 4 (over y), kv: 32 (over z, x), tp: 2 (over core).
Axes of the slice: x: 4, y: 4, z: 8, core: 2. Of those that a mesh axis runs over, the one named last changes fastest.
Arguments:
- tokens: bfloat16 [16, 16, 2048], P('dp', None, 'kv'), may hold values from -6 to 6
- norm_gain: float32 [2048], P('kv'), may hold values from 0.1 to 1.9
- w_query: bfloat16 [2048, 1024], P('kv', 'tp'), may hold values from -0.125 to 0.125
- w_key: bfloat16 [2048, 1024], P('kv', 'tp'), may hold values from -0.125 to 0.125
- w_value: bfloat16 [2048, 1024], P('kv', 'tp'), may hold values from -0.125 to 0.125
- w_forget: bfloat16 [2048, 16], replicated, may hold values from -0.125 to 0.125
- forget_bias: float32 [16], replicated, may hold values from -2 to 4
- query_gain: float32 [64], replicated, may hold values from 0.1 to 1.9
- key_gain: float32 [64], replicated, may hold values from 0.1 to 1.9
- head_gain: float32 [64], replicated, may hold values from 0.1 to 1.9
- w_out: bfloat16 [1024, 2048], P('tp', 'kv'), may hold values from -0.1875 to 0.1875
- key_cache: bfloat16 [16, 16384, 1024], P('dp', 'kv', 'tp'), may hold values from -240 to 240
- value_cache: bfloat16 [16, 16384, 1024], P('dp', 'kv', 'tp'), may hold values from -6 to 6
- gate_cache: float32 [16, 16, 16384], P('dp', 'tp', 'kv'), may hold values from -1922 to 0, as said below
- lengths: int32 [16], P('dp'), may hold values from 15341 to 16364
- accepted: int32 [16], P('dp'), may hold values from 0 to 4
- parents: int32 [16, 16], P('dp'), may hold values from -1 to 14, as said below
Outputs:
- layer_out: bfloat16 [16, 16, 2048], P('dp', None, 'kv')
- new_keys: bfloat16 [16, 16384, 1024], P('dp', 'kv', 'tp')
- new_values: bfloat16 [16, 16384, 1024], P('dp', 'kv', 'tp')
- proposal_gates: float32 [16, 16, 16], P('dp', None, 'tp')
The draws below stay inside these ranges and needn't reach their ends.
Inputs may be any that keep to these rules, and one draw needn't show every extreme that they name: `gate_cache`: each entry is the running sum of log forget gates up to its position, so entries never rise along positions; entries at and after lengths hold the last step's proposals in order. `parents`: proposal 0 follows the last accepted token (parent -1); every other proposal's parent is one of the three proposals before it.
All inputs are finite; a program needn't handle non-finite values.
Results may differ from the reference program's by a relative error of at most 0.0051.
The reference program's roundings to bfloat16 on the way (of `scaled`, `values_new` and `normed`) count: a program that leaves them out, or rounds other values in their place, can miss the bound.
Values may be sent and summed in bfloat16 or wider, within the bound.
A program may use at most 64 MiB of HBM per device.

```python
import jax
import jax.numpy as jnp
from jax import lax

D = 2048
HEADS = 16
DH = 64
PROPS = 16
ACCEPT_MOST = 4
POS_DEV = 512
HW = 1024
HEAD_GROUP = 8
SEQUENCE_TOTAL = 16
CACHE_POSITIONS = 16384
N_KV = 32
N_TP = 2


def draw_key_cache(key, part):
    key_one = jax.random.fold_in(key, 0)
    entries = jnp.clip(jax.random.normal(key_one, (SEQUENCE_TOTAL, CACHE_POSITIONS, HEADS * DH), jnp.float32), -6.0, 6.0)
    return entries.astype(jnp.bfloat16)


def draw_gate_cache(key, part):
    every_key = jax.random.split(key, 7)
    slow_share = 0.5
    slow_heads = jax.random.uniform(every_key[0], (SEQUENCE_TOTAL, HEADS, 1)) < slow_share
    slow_rate = jax.random.uniform(every_key[1], (SEQUENCE_TOTAL, HEADS, 1), minval=0.2, maxval=0.8) / CACHE_POSITIONS
    fast_rate = 1.0 / (POS_DEV * jax.random.uniform(every_key[2], (SEQUENCE_TOTAL, HEADS, 1), minval=0.06, maxval=0.2))
    decay_rates = jnp.where(slow_heads, slow_rate, fast_rate)
    block_multiplier = jnp.exp(jax.random.uniform(every_key[3], (SEQUENCE_TOTAL, HEADS, CACHE_POSITIONS // POS_DEV), minval=-0.7, maxval=0.7))
    block_multiplier = jnp.repeat(block_multiplier, POS_DEV, axis=2)
    coarse_estimate = jax.random.uniform(every_key[4], (SEQUENCE_TOTAL, HEADS, CACHE_POSITIONS), minval=0.3, maxval=1.7)
    flurry_position = jax.random.randint(every_key[5], (SEQUENCE_TOTAL, 1, 2), 0, CACHE_POSITIONS)
    position_numbers = jnp.arange(CACHE_POSITIONS, dtype=jnp.int32)[None, None, :]
    flurry_groups = ((position_numbers == flurry_position[..., 0:1]) | (position_numbers == flurry_position[..., 1:2])).astype(jnp.float32)
    tree_depth = jax.random.uniform(every_key[6], (SEQUENCE_TOTAL, HEADS, 1), minval=0.22, maxval=0.69)
    logarithm_gates = -decay_rates * block_multiplier * coarse_estimate - flurry_groups * tree_depth
    return jnp.cumsum(logarithm_gates, axis=2).astype(jnp.float32)


def draw_parents(key, part):
    draws = jax.random.randint(key, (SEQUENCE_TOTAL, PROPS), 0, 3, dtype=jnp.int32)
    step_ids = jnp.arange(PROPS, dtype=jnp.int32)[None, :]
    back_steps = draws % jnp.maximum(jnp.minimum(step_ids, 3), 1)
    return jnp.where(step_ids == 0, -1, step_ids - 1 - back_steps).astype(jnp.int32)


def with_ends(values, key, low, high):
    longest = values.shape.index(max(values.shape))
    spots = []
    for shift in (0, 1):
        where = [jax.random.randint(jax.random.fold_in(key, axis), (), 0, length) for axis, length in enumerate(values.shape)]
        where[longest] = (where[longest] + shift) % values.shape[longest]
        spots.append(tuple(where))
    return values.at[spots[0]].set(low).at[spots[1]].set(high)


def block_levels(rng, shape, cuts, low, top_value):
    level, own = 1.0, jax.random.fold_in(rng, 6)
    for axis_at, shards_of in cuts:
        heights = jnp.exp(jax.random.uniform(jax.random.fold_in(own, axis_at), (shards_of,), jnp.float32, low / len(cuts), top_value / len(cuts)))
        level = level * jnp.repeat(heights, shape[axis_at] // shards_of).reshape([-1 if axis == axis_at else 1 for axis in range(len(shape))])
    return level


def gaussian(key, dims, width, most, shards=(), kind=jnp.bfloat16):
    gain = block_levels(key, dims, shards, -0.22, 0.18) if shards else 1.0
    drawn = jax.random.normal(key, dims, jnp.float32) * width * gain
    return jnp.minimum(jnp.maximum(drawn, -most), most).astype(kind)


def setup_inputs(seed: int = 0) -> dict:
    arg_keys = jax.random.split(jax.random.key(seed), 18)
    tokens = gaussian(arg_keys[0], (SEQUENCE_TOTAL, PROPS, D), 1.0, 6.0, ((0, 4), (2, 32)))
    norm_gain = jnp.clip(1.0 + 0.18 * jax.random.normal(arg_keys[1], (D,), jnp.float32), 0.1, 1.9)
    w_query = gaussian(arg_keys[2], (D, HW), D ** -0.5, 0.125, ((0, 32), (1, 2)))
    w_key = gaussian(arg_keys[3], (D, HW), D ** -0.5, 0.125, ((0, 32), (1, 2)))
    w_value = gaussian(arg_keys[4], (D, HW), D ** -0.5, 0.125, ((0, 32), (1, 2)))
    w_forget = gaussian(arg_keys[5], (D, HEADS), D ** -0.5, 0.125)
    forget_bias = jnp.clip(jax.random.uniform(arg_keys[6], (HEADS,), jnp.float32, -2.0, 4.0), -2.0, 4.0)
    query_gain = jnp.clip(1.0 + 0.18 * jax.random.normal(arg_keys[7], (DH,), jnp.float32), 0.1, 1.9)
    key_gain = jnp.clip(1.0 + 0.18 * jax.random.normal(arg_keys[8], (DH,), jnp.float32), 0.1, 1.9)
    head_gain = jnp.clip(1.0 + 0.18 * jax.random.normal(arg_keys[9], (DH,), jnp.float32), 0.1, 1.9)
    w_out = gaussian(arg_keys[10], (HW, D), HW ** -0.5, 0.1875, ((0, 2), (1, 32)))
    key_cache = draw_key_cache(jax.random.fold_in(arg_keys[17], 71), 0)
    value_cache = gaussian(arg_keys[12], (SEQUENCE_TOTAL, CACHE_POSITIONS, HW), 1.0, 6.0, ((0, 4), (1, 32), (2, 2)))
    gate_cache = draw_gate_cache(jax.random.fold_in(arg_keys[17], 71), 0)
    lengths = with_ends(jax.random.randint(arg_keys[14], (SEQUENCE_TOTAL,), CACHE_POSITIONS - PROPS - ACCEPT_MOST + 1 - 2 * POS_DEV, CACHE_POSITIONS - PROPS - ACCEPT_MOST + 1), jax.random.fold_in(arg_keys[14], 1), CACHE_POSITIONS - PROPS - ACCEPT_MOST + 1 - 2 * POS_DEV, CACHE_POSITIONS - PROPS - ACCEPT_MOST).astype(jnp.int32)
    accepted = with_ends(jax.random.randint(arg_keys[15], (SEQUENCE_TOTAL,), 0, ACCEPT_MOST + 1), jax.random.fold_in(arg_keys[15], 1), 0, ACCEPT_MOST).astype(jnp.int32)
    parents = draw_parents(jax.random.fold_in(arg_keys[17], 71), 0)
    return dict(tokens=tokens, norm_gain=norm_gain, w_query=w_query, w_key=w_key, w_value=w_value, w_forget=w_forget, forget_bias=forget_bias, query_gain=query_gain, key_gain=key_gain, head_gain=head_gain, w_out=w_out, key_cache=key_cache, value_cache=value_cache, gate_cache=gate_cache, lengths=lengths, accepted=accepted, parents=parents)


EPSILON = 1e-06
MASKED = -1e+30

def head_norm(head_rows, gain_vec):
    mean_square = lax.optimization_barrier(jnp.mean(head_rows * head_rows, axis=-1, keepdims=True))
    return head_rows * lax.rsqrt(mean_square + EPSILON) * gain_vec

def ancestry(parents):
    count_all = parents.shape[0]
    step_ids = jnp.arange(count_all, dtype=jnp.int32)
    step_matrix = (parents[:, None] == step_ids[None, :]).astype(jnp.float32)
    identity = jnp.eye(count_all, dtype=jnp.float32)

    def extend(turn_index, ancestors):
        return identity + jnp.dot(step_matrix, ancestors, precision=lax.Precision.HIGHEST)
    return lax.fori_loop(0, count_all, extend, identity)

def softmax_block(scores, live_mask, block_values):
    row_max = lax.optimization_barrier(jnp.max(scores, axis=-1))
    weights = jnp.where(live_mask, jnp.exp(scores - row_max[..., None]), 0.0)
    row_total = lax.optimization_barrier(jnp.sum(weights, axis=-1))
    rounded = lax.optimization_barrier(weights.astype(jnp.bfloat16)).astype(jnp.float32)
    weighted = jnp.einsum('hpk,khd->phd', rounded, block_values.astype(jnp.float32))
    return (row_max.T, row_total.T, weighted)

def combine(earlier, later):
    earlier_max, earlier_total, earlier_sum = earlier
    later_max, later_total, later_sum = later
    row_max = jnp.maximum(earlier_max, later_max)
    earlier_scale = jnp.exp(earlier_max - row_max)
    later_scale = jnp.exp(later_max - row_max)
    return (row_max, earlier_total * earlier_scale + later_total * later_scale, earlier_sum * earlier_scale[..., None] + later_sum * later_scale[..., None])

def one_sequence(items, shared):
    tokens, key_cache, value_cache, gate_cache, length, accept, parents = items
    norm_gain, w_query, w_key, w_value, w_forget, forget_bias, query_gain, key_gain, head_gain, w_out = shared
    token_rows = tokens.astype(jnp.float32)
    inverse = lax.rsqrt(lax.optimization_barrier(jnp.mean(token_rows * token_rows, axis=1)) + EPSILON)[:, None]
    scaled = (token_rows * norm_gain).astype(jnp.bfloat16)
    query_raw = jnp.dot(scaled, w_query, preferred_element_type=jnp.float32) * inverse
    key_raw = jnp.dot(scaled, w_key, preferred_element_type=jnp.float32) * inverse
    value_raw = jnp.dot(scaled, w_value, preferred_element_type=jnp.float32) * inverse
    gate_raw = jnp.dot(scaled, w_forget, preferred_element_type=jnp.float32) * inverse
    queries = head_norm(query_raw.reshape(PROPS, HEADS, DH), query_gain).astype(jnp.bfloat16)
    keys_new = head_norm(key_raw.reshape(PROPS, HEADS, DH), key_gain).astype(jnp.bfloat16)
    values_new = value_raw.astype(jnp.bfloat16).reshape(PROPS, HEADS, DH)
    logarithm_gates = jax.nn.log_sigmoid(gate_raw + forget_bias)
    ancestors = ancestry(parents)
    path_sum = jnp.dot(ancestors, logarithm_gates, precision=lax.Precision.HIGHEST)
    base_pos = length + accept
    boundary = lax.dynamic_slice_in_dim(gate_cache, base_pos - 1, 1, 1)[:, 0]
    score_scale = DH ** (-0.5)
    score_shift = boundary[:, None, None] + path_sum.T[:, :, None]
    key_blocks = key_cache.reshape(N_KV, POS_DEV, HEADS, DH)
    value_blocks = value_cache.reshape(N_KV, POS_DEV, HEADS, DH)
    gate_blocks = gate_cache.reshape(HEADS, N_KV, POS_DEV).transpose(1, 0, 2)
    block_starts = jnp.arange(N_KV, dtype=jnp.int32) * POS_DEV
    query_wide = queries.astype(jnp.float32)

    def cache_block(block_args):
        block_keys, block_values, block_gates, block_start = block_args
        scores = jnp.einsum('phd,khd->hpk', query_wide, block_keys.astype(jnp.float32)) * score_scale
        scores = scores + score_shift - block_gates[:, None, :]
        live_mask = (block_start + jnp.arange(POS_DEV, dtype=jnp.int32) < base_pos)[None, None, :]
        scores = jnp.where(live_mask, scores, MASKED)
        return softmax_block(scores, live_mask, block_values)
    block_max, block_total, block_sum = lax.map(cache_block, (key_blocks, value_blocks, gate_blocks, block_starts))
    row_max = lax.optimization_barrier(jnp.max(block_max, axis=0))
    factors = jnp.exp(block_max - row_max)
    cache_part = (row_max, lax.optimization_barrier(jnp.sum(block_total * factors, axis=0)), lax.optimization_barrier(jnp.sum(block_sum * factors[..., None], axis=0)))
    tree_scores = jnp.einsum('phd,jhd->hpj', query_wide, keys_new.astype(jnp.float32)) * score_scale
    tree_scores = tree_scores + path_sum.T[:, :, None] - path_sum.T[:, None, :]
    tree_live = (ancestors > 0.5)[None]
    tree_scores = jnp.where(tree_live, tree_scores, MASKED)
    tree_part = softmax_block(tree_scores, tree_live, values_new)
    row_max, row_total, weighted = combine(cache_part, tree_part)
    attended = weighted / row_total[..., None]
    normed = head_norm(attended, head_gain).astype(jnp.bfloat16).reshape(PROPS, HW)
    group_width = HEAD_GROUP * DH
    layer_sum = jnp.zeros((PROPS, D), jnp.float32)
    for group_index in range(N_TP):
        lower = group_index * group_width
        group_term = jnp.dot(normed[:, lower:lower + group_width], w_out[lower:lower + group_width], preferred_element_type=jnp.float32)
        layer_sum = layer_sum + lax.optimization_barrier(group_term.astype(jnp.bfloat16)).astype(jnp.float32)
    layer_out = layer_sum.astype(jnp.bfloat16)
    zero_index = jnp.zeros((), jnp.int32)
    new_keys = lax.dynamic_update_slice(key_cache, keys_new.reshape(PROPS, HW), (base_pos, zero_index))
    new_values = lax.dynamic_update_slice(value_cache, values_new.reshape(PROPS, HW), (base_pos, zero_index))
    return (layer_out, new_keys, new_values, logarithm_gates)

def reference(tokens, norm_gain, w_query, w_key, w_value, w_forget, forget_bias, query_gain, key_gain, head_gain, w_out, key_cache, value_cache, gate_cache, lengths, accepted, parents):
    shared = (norm_gain, w_query, w_key, w_value, w_forget, forget_bias, query_gain, key_gain, head_gain, w_out)

    def per_sequence(items):
        return one_sequence(items, shared)
    layer_out, new_keys, new_values, proposal_gates = lax.map(per_sequence, (tokens, key_cache, value_cache, gate_cache, lengths, accepted, parents))
    return (layer_out, new_keys, new_values, proposal_gates)
```

```python
import functools

import jax
import jax.numpy as jnp
from jax import lax
from jax.experimental import pallas as pl
from jax.experimental.pallas import tpu as pltpu
from jax.sharding import PartitionSpec as P

EPSILON = 1e-06
MASKED = -1e30
MESH = pl.DeviceIdType.MESH
F32 = jnp.float32
BF16 = jnp.bfloat16

NZ, NX = 8, 4
N_KV = NZ * NX
SEQS, PROPS, HEADS, DH = 4, 16, 8, 64
ROWS = SEQS * PROPS
WIDTH = HEADS * DH
POS = 512
D = 2048
FEATS = D // N_KV
LANES = 128
FIRST_OWNER = 15341 // POS
CHUNK = 128
QN, GL, KVN, PS, NR, WO = 3, 7, 8, 9, 11, 15

OFFSETS = sorted(
    ((dz, dx) for dz in range(NZ) for dx in range(NX) if (dz, dx) != (0, 0)),
    key=lambda o: -(min(o[0], NZ - o[0]) + min(o[1], NX - o[1])),
)


def iota(shape, dim):
    return lax.broadcasted_iota(jnp.int32, shape, dim)


def swap(x):
    return pltpu.roll(x, DH, 1)


def dot(a, b, dims, precision=None):
    return lax.dot_general(
        a, b, (dims, ((), ())), preferred_element_type=F32, precision=precision
    )


def layer_kernel(
    tokens,
    norm_gain,
    w_query,
    w_key,
    w_value,
    w_forget,
    forget_bias,
    query_gain,
    key_gain,
    head_gain,
    w_out,
    key_cache,
    value_cache,
    gate_cache,
    lengths,
    accepted,
    parents,
    out_ref,
    gates_ref,
    kvn_ref,
    tok_v,
    w_v,
    wf_v,
    wo_v,
    ng_v,
    qg_v,
    kg_v,
    hg_v,
    par_v,
    fb_s,
    len_s,
    acc_s,
    k_v,
    v_v,
    g_v,
    q_send,
    q_recv,
    st_send,
    st_recv,
    kv_send,
    kv_recv,
    qn_send,
    qn_recv,
    kvn_send,
    kvn_recv,
    gl_send,
    gl_recv,
    p_send,
    p_recv,
    ps_send,
    ps_recv,
    n_send,
    n_recv,
    load_sem,
    ssem,
    rsem,
):
    me = lax.axis_index("kv")
    tp = lax.axis_index("tp")
    mz, mx = me // NX, me % NX
    peers = [((mz + dz) % NZ) * NX + (mx + dx) % NX for dz, dx in OFFSETS]
    s_me, h_me = me // HEADS, me % HEADS

    loads = []

    def load(src, dst):
        copy = pltpu.make_async_copy(src, dst, load_sem.at[len(loads)])
        copy.start()
        loads.append(copy)
        return copy

    first = [
        load(tokens, tok_v),
        load(norm_gain, ng_v),
        load(w_query, w_v.at[:, pl.ds(0, WIDTH)]),
        load(w_forget.at[:, pl.ds(pl.multiple_of(me // 2 * LANES, LANES), LANES)], wf_v),
        load(w_key, w_v.at[:, pl.ds(WIDTH, WIDTH)]),
        load(w_value, w_v.at[:, pl.ds(2 * WIDTH, WIDTH)]),
    ]
    barrier = pltpu.get_barrier_semaphore()
    for p in peers:
        for core in range(2):
            pl.semaphore_signal(
                barrier, inc=1, device_id={"kv": p, "tp": core}, device_id_type=MESH
            )
    pl.semaphore_signal(barrier, inc=1, device_id={"tp": 1 - tp}, device_id_type=MESH)
    small = [
        load(parents, par_v),
        load(forget_bias, fb_s),
        load(query_gain, qg_v),
        load(key_gain, kg_v),
        load(head_gain, hg_v),
        load(lengths, len_s),
        load(accepted, acc_s),
    ]
    out_load = load(w_out, wo_v.at[tp])
    cached = [load(key_cache, k_v), load(value_cache, v_v), load(gate_cache, g_v)]

    def send(src, dst, phase, kv, core=None, recv=None):
        pltpu.make_async_remote_copy(
            src_ref=src,
            dst_ref=dst,
            send_sem=ssem.at[phase],
            recv_sem=rsem.at[phase if recv is None else recv],
            device_id={"kv": kv} if core is None else {"kv": kv, "tp": core},
            device_id_type=MESH,
        ).start()

    def await_recv(buf, phase, count):
        part = buf.at[pl.ds(0, count)]
        pltpu.make_async_remote_copy(
            src_ref=part,
            dst_ref=part,
            send_sem=ssem.at[phase],
            recv_sem=rsem.at[phase],
            device_id={"kv": peers[0]},
            device_id_type=MESH,
        ).wait_recv()

    def await_send(buf, phase, count):
        part = buf.at[pl.ds(0, count)]
        pltpu.make_async_remote_copy(
            src_ref=part,
            dst_ref=part,
            send_sem=ssem.at[phase],
            recv_sem=rsem.at[phase],
            device_id={"kv": peers[0]},
            device_id_type=MESH,
        ).wait_send()

    low8 = iota((8, LANES), 1) < DH
    low16 = iota((16, LANES), 1) < DH

    for copy in first:
        copy.wait()
    rows = tok_v[...].reshape(ROWS, FEATS).astype(F32)
    scaled = (rows * ng_v[...].reshape(1, FEATS)).astype(BF16)
    summed = dot(scaled, w_v[...], ((1,), (0,)))
    forget = wf_v[...].astype(F32)
    forget = jnp.where(me % 2 == 1, swap(forget), forget)[:, :FEATS].astype(BF16)
    gate_part = dot(forget, scaled, ((1,), (1,)))
    squares = dot(
        jnp.ones((2 * HEADS, FEATS), F32), rows * rows, ((1,), (1,)), lax.Precision.HIGHEST
    )
    st_send[...] = jnp.concatenate([gate_part, squares], axis=1).reshape(2 * HEADS, 1, LANES)
    for s in range(SEQS):
        for t in range(HEADS // 2):
            a = summed[s * 16 : s * 16 + 8, t * LANES : (t + 1) * LANES]
            b = summed[s * 16 + 8 : s * 16 + 16, t * LANES : (t + 1) * LANES]
            q_send[s * HEADS + 2 * t] = jnp.where(low8, a, swap(b))
            q_send[s * HEADS + 2 * t + 1] = jnp.where(low8, swap(a), b)
    for s in range(SEQS):
        for t in range(HEADS // 2):
            at = WIDTH + t * LANES
            k = summed[s * 16 : s * 16 + 16, at : at + LANES]
            v = summed[s * 16 : s * 16 + 16, at + WIDTH : at + WIDTH + LANES]
            kv_send[s * HEADS + 2 * t] = jnp.where(low16, k, swap(v)).astype(BF16)
            kv_send[s * HEADS + 2 * t + 1] = jnp.where(low16, swap(k), v).astype(BF16)

    pl.semaphore_wait(barrier, 2 * N_KV - 1)

    for p in peers:
        send(q_send.at[p], q_recv.at[me], 0, p)
        send(st_send.at[tp * HEADS + p % HEADS], st_recv.at[me], 1, p)
    for p in peers:
        send(kv_send.at[p], kv_recv.at[me], 2, p)
    q_recv[me] = q_send[me]
    st_recv[me] = st_send[tp * HEADS + h_me]
    kv_recv[me] = kv_send[me]

    for copy in small:
        copy.wait()
    out_load.wait()
    send(wo_v.at[tp], wo_v.at[tp], WO, me, 1 - tp)

    parent_row = par_v[pl.ds(s_me, 1), :]
    step_t = (iota((PROPS, PROPS), 0) == parent_row).astype(BF16)
    eye = (iota((PROPS, PROPS), 0) == iota((PROPS, PROPS), 1)).astype(F32)
    ancestors_t = eye + step_t.astype(F32)
    power = step_t
    for _ in range(3):
        power = dot(power, power, ((1,), (0,))).astype(BF16)
        ancestors_t = ancestors_t + dot(ancestors_t.astype(BF16), power, ((1,), (0,)))
    ancestors = ancestors_t.T

    await_recv(st_recv, 1, N_KV - 1)
    stats = jnp.sum(st_recv[...].reshape(N_KV, LANES), axis=0, keepdims=True)
    inverse_row = lax.rsqrt(stats / D + EPSILON)
    logits = stats * swap(inverse_row) + fb_s[tp * HEADS + h_me]
    log_row = jnp.minimum(logits, 0.0) - jnp.log1p(jnp.exp(-jnp.abs(logits)))
    spot = s_me * PROPS
    at_row = iota((PROPS, LANES), 0) + spot
    at_lane = iota((PROPS, LANES), 1)
    inverse = jnp.sum(
        jnp.where(at_lane == at_row + ROWS, inverse_row, 0.0), axis=1, keepdims=True
    )
    own_log = jnp.sum(jnp.where(at_lane == at_row, log_row, 0.0), axis=1, keepdims=True)
    path_row = jnp.sum(ancestors_t * own_log, axis=0, keepdims=True)
    gl_send[...] = log_row

    await_recv(q_recv, 0, N_KV - 1)
    raw = jnp.sum(q_recv[...], axis=0) * jnp.where(low8, inverse[:8], inverse[8:])
    gain = qg_v[...].reshape(1, DH)
    gain = jnp.concatenate([gain, gain], axis=1)
    square = raw * raw
    mean_low = jnp.sum(jnp.where(low8, square, 0.0), axis=1, keepdims=True) / DH
    mean_high = jnp.sum(jnp.where(low8, 0.0, square), axis=1, keepdims=True) / DH
    q_packed = (raw * lax.rsqrt(jnp.where(low8, mean_low, mean_high) + EPSILON) * gain).astype(
        BF16
    )
    qn_send[...] = q_packed

    for p in peers:
        send(qn_send, qn_recv.at[me], QN, p, recv=QN + s_me)
    qn_recv[me] = q_packed

    @pl.when(s_me == 0)
    def _():
        for p in peers:
            send(gl_send, gl_recv.at[h_me], GL, p)
        gl_recv[h_me] = log_row

    await_recv(kv_recv, 2, N_KV - 1)
    raw_kv = jnp.sum(kv_recv[...].astype(F32), axis=0) * inverse
    mean_key = jnp.sum(jnp.where(low16, raw_kv * raw_kv, 0.0), axis=1, keepdims=True) / DH
    gain = kg_v[...].reshape(1, DH)
    gain = jnp.concatenate([gain, gain], axis=1)
    kv_new = jnp.where(low16, raw_kv * lax.rsqrt(mean_key + EPSILON) * gain, raw_kv).astype(BF16)
    kvn_send[...] = kv_new
    for owner in range(FIRST_OWNER, N_KV):

        @pl.when(me != owner)
        def _():
            send(kvn_send, kvn_recv.at[me], KVN, owner)

        @pl.when(me == owner)
        def _():
            kvn_recv[me] = kv_new

    q32 = q_packed.astype(F32)
    q_rows = jnp.concatenate(
        [jnp.where(low8, q32, 0.0), jnp.where(low8, swap(q32), 0.0)], axis=0
    ).astype(BF16)
    tree = dot(q_rows, kv_new, ((1,), (1,))) * DH**-0.5 - path_row
    tree_live = ancestors > 0.5
    tree = jnp.where(tree_live, tree, MASKED)
    tree_max = jnp.max(tree, axis=1, keepdims=True)
    tree_weights = jnp.where(tree_live, jnp.exp(tree - tree_max), 0.0)
    tree_total = jnp.sum(tree_weights, axis=1, keepdims=True)
    tree_sum = dot(tree_weights.astype(BF16), kv_new, ((1,), (0,)))
    tree_packed = jnp.where(low8, swap(tree_sum[:8]), tree_sum[8:])

    for copy in cached:
        copy.wait()
    pos = iota((1, POS), 1) + me * POS
    diag = iota((PROPS, LANES), 1) - iota((PROPS, LANES), 0)
    corner = (iota((PROPS, LANES), 0) == 0) & (iota((PROPS, LANES), 1) == 2 * PROPS)
    for turn in (0, 1, 3, 2):
        s = (s_me + turn) % SEQS
        await_recv(qn_recv, QN + s, HEADS if turn else HEADS - 1)
        base = len_s[s] + acc_s[s]
        live = pos < base
        gates = g_v[s]
        bound = jnp.sum(jnp.where(pos == base - 1, gates, 0.0), axis=1, keepdims=True)
        for t in range(HEADS // 2):
            m0 = qn_recv[s * HEADS + 2 * t].astype(F32)
            m1 = qn_recv[s * HEADS + 2 * t + 1].astype(F32)
            lhs = jnp.concatenate(
                [
                    jnp.where(low8, m0, 0.0),
                    jnp.where(low8, swap(m0), 0.0),
                    jnp.where(low8, 0.0, swap(m1)),
                    jnp.where(low8, 0.0, m1),
                ],
                axis=0,
            ).astype(BF16)
            keys = k_v[s, :, pl.ds(t * LANES, LANES)]
            values = v_v[s, :, pl.ds(t * LANES, LANES)]
            scores = dot(lhs, keys, ((1,), (1,))) * DH**-0.5
            gate_rows = jnp.concatenate(
                [
                    jnp.broadcast_to(gates[2 * t : 2 * t + 1], (PROPS, POS)),
                    jnp.broadcast_to(gates[2 * t + 1 : 2 * t + 2], (PROPS, POS)),
                ],
                axis=0,
            )
            scores = jnp.where(live, scores - gate_rows, MASKED)
            peak = jnp.max(scores, axis=1, keepdims=True)
            weights = jnp.where(live, jnp.exp(scores - peak), 0.0)
            total = jnp.sum(weights, axis=1, keepdims=True)
            part = dot(weights.astype(BF16), values, ((1,), (0,)))
            p_send[s * HEADS + 2 * t] = jnp.where(low8, part[:8], swap(part[8:16]))
            p_send[s * HEADS + 2 * t + 1] = jnp.where(low8, swap(part[16:24]), part[24:32])
            for odd in range(2):
                rows_at = slice(odd * PROPS, (odd + 1) * PROPS)
                head = 2 * t + odd
                tile = jnp.where(diag == 0, peak[rows_at], 0.0)
                tile = jnp.where(diag == PROPS, total[rows_at], tile)
                tile = jnp.where(corner, bound[head : head + 1], tile)
                ps_send[s * HEADS + head] = jnp.sum(tile, axis=0, keepdims=True)
        for j in range(HEADS):
            if turn == 0 and j == 0:
                continue
            target = s * HEADS + (h_me + j) % HEADS
            send(p_send.at[target], p_recv.at[me], PS, target)
            send(ps_send.at[target], ps_recv.at[me], PS + 1, target)
    p_recv[me] = p_send[me]
    ps_recv[me] = ps_send[me]

    await_recv(ps_recv, PS + 1, N_KV - 1)
    stats_t = ps_recv[...].reshape(N_KV, LANES).T
    peaks = stats_t[:PROPS]
    bound = jnp.sum(stats_t[2 * PROPS : 2 * PROPS + 1], axis=1, keepdims=True)
    tree_max = tree_max - bound
    top = jnp.maximum(jnp.max(peaks, axis=1, keepdims=True), tree_max)
    factors = jnp.exp(peaks - top)
    tree_factor = jnp.exp(tree_max - top)
    total = (
        jnp.sum(factors * stats_t[PROPS : 2 * PROPS], axis=1, keepdims=True)
        + tree_total * tree_factor
    )
    await_recv(p_recv, PS, N_KV - 1)
    acc = [tree_packed * jnp.where(low8, tree_factor[:8], tree_factor[8:])] + [None] * 3
    for i in range(N_KV):
        factor = jnp.where(low8, factors[:8, i : i + 1], factors[8:, i : i + 1])
        term = p_recv[i] * factor
        acc[i % 4] = term if acc[i % 4] is None else acc[i % 4] + term
    weighted = (acc[0] + acc[1]) + (acc[2] + acc[3])
    attended = weighted / jnp.where(low8, total[:8], total[8:])
    square = attended * attended
    mean_low = jnp.sum(jnp.where(low8, square, 0.0), axis=1, keepdims=True) / DH
    mean_high = jnp.sum(jnp.where(low8, 0.0, square), axis=1, keepdims=True) / DH
    gain = hg_v[...].reshape(1, DH)
    gain = jnp.concatenate([gain, gain], axis=1)
    normed = (
        attended * lax.rsqrt(jnp.where(low8, mean_low, mean_high) + EPSILON) * gain
    ).astype(BF16)
    n_send[...] = normed

    slot = tp * N_KV + me
    for p in peers:
        for core in range(2):
            send(n_send, n_recv.at[slot], NR, p, core, recv=NR + s_me)
    send(n_send, n_recv.at[slot], NR, me, 1 - tp, recv=NR + s_me)
    n_recv[slot] = normed

    @pl.when(s_me == 0)
    def _():
        await_recv(gl_recv, GL, HEADS - 1)

    @pl.when(s_me != 0)
    def _():
        await_recv(gl_recv, GL, HEADS)

    logs = gl_recv[...].reshape(HEADS, LANES)
    for s in range(SEQS):
        gates_ref[s] = logs[:, s * PROPS : (s + 1) * PROPS]

    @pl.when(me >= FIRST_OWNER)
    def _():
        await_recv(kvn_recv, KVN, N_KV - 1)
        kvn_ref[...] = kvn_recv[...]

    @pl.when(me < FIRST_OWNER)
    def _():
        kvn_ref[...] = jnp.zeros_like(kvn_ref)

    await_recv(wo_v, WO, 1)
    for turn in (0, 1, 3, 2):
        s = (s_me + turn) % SEQS
        await_recv(n_recv, NR + s, 2 * HEADS if turn else 2 * HEADS - 1)
        layer_sum = None
        for core in range(2):
            tiles = []
            for t in range(HEADS // 2):
                m0 = n_recv[core * N_KV + s * HEADS + 2 * t].astype(F32)
                m1 = n_recv[core * N_KV + s * HEADS + 2 * t + 1].astype(F32)
                tiles.append(
                    jnp.concatenate(
                        [jnp.where(low8, m0, swap(m1)), jnp.where(low8, swap(m0), m1)], axis=0
                    ).astype(BF16)
                )
            term = dot(jnp.concatenate(tiles, axis=1), wo_v[core], ((1,), (1,)))
            term = term.astype(BF16).astype(F32)
            layer_sum = term if layer_sum is None else layer_sum + term
        out_ref[s] = layer_sum.astype(BF16)

    await_send(q_send, 0, N_KV - 1)
    await_send(st_recv, 1, N_KV - 1)
    await_send(kv_send, 2, N_KV - 1)
    await_send(qn_recv, QN, N_KV - 1)
    await_send(wo_v, WO, 1)

    @pl.when(s_me == 0)
    def _():
        await_send(st_recv, GL, N_KV - 1)

    @pl.when(me >= FIRST_OWNER)
    def _():
        await_send(kvn_recv, KVN, N_KV - FIRST_OWNER - 1)

    @pl.when(me < FIRST_OWNER)
    def _():
        await_send(kvn_recv, KVN, N_KV - FIRST_OWNER)

    await_send(p_send, PS, N_KV - 1)
    await_send(ps_send, PS + 1, N_KV - 1)
    await_send(n_recv, NR, 2 * N_KV - 1)


def cache_kernel(
    key_cache,
    value_cache,
    kvn,
    lengths,
    accepted,
    layer_in,
    gates_in,
    layer_out,
    new_keys,
    new_values,
    gates_out,
    k_v,
    v_v,
    sem,
):
    me = lax.axis_index("kv")
    sides = ((key_cache, k_v, new_keys), (value_cache, v_v, new_values))
    ends = [
        pltpu.make_async_copy(layer_in, layer_out, sem.at[0]),
        pltpu.make_async_copy(gates_in, gates_out, sem.at[1]),
    ]

    def write(s, c, side, patched):
        src, buf, dst = sides[side]
        rows = pl.ds(pl.multiple_of(c * CHUNK, CHUNK), CHUNK)
        return pltpu.make_async_copy(
            (buf if patched else src).at[s, rows], dst.at[s, rows], sem.at[2 + s]
        )

    for s in range(SEQS):
        offset = lengths[s] + accepted[s] - me * POS
        for c in range(POS // CHUNK):
            clear = (offset >= (c + 1) * CHUNK) | (offset + PROPS <= c * CHUNK)

            @pl.when(clear)
            def _():
                for side in range(2):
                    write(s, c, side, False).start()

    for copy in ends:
        copy.start()
    low = iota((CHUNK, LANES), 1) < DH

    @pl.when(me >= FIRST_OWNER)
    def _():
        for s in range(SEQS):
            offset = lengths[s] + accepted[s] - me * POS

            def patch(c):
                slot = iota((CHUNK, 1), 0) + c * CHUNK - offset
                hit = (slot >= 0) & (slot < PROPS)
                placing = (slot == iota((CHUNK, PROPS), 1)).astype(BF16)
                rows = pl.ds(pl.multiple_of(c * CHUNK, CHUNK), CHUNK)
                for t in range(HEADS // 2):
                    w0 = dot(placing, kvn[s * HEADS + 2 * t], ((1,), (0,)))
                    w1 = dot(placing, kvn[s * HEADS + 2 * t + 1], ((1,), (0,)))
                    at = (s, rows, pl.ds(t * LANES, LANES))
                    k_v[at] = jnp.where(
                        hit, jnp.where(low, w0, swap(w1)), key_cache[at].astype(F32)
                    ).astype(BF16)
                    v_v[at] = jnp.where(
                        hit, jnp.where(low, swap(w0), w1), value_cache[at].astype(F32)
                    ).astype(BF16)
                for side in range(2):
                    write(s, c, side, True).start()

            first = jnp.maximum(offset, 0) // CHUNK
            last = jnp.minimum(offset + PROPS - 1, POS - 1) // CHUNK

            @pl.when((offset > -PROPS) & (offset < POS))
            def _():
                patch(first)

                @pl.when(last > first)
                def _():
                    patch(last)

    for s in range(SEQS):
        for src, _, dst in sides:
            pltpu.make_async_copy(src.at[s], dst.at[s], sem.at[2 + s]).wait()
    for copy in ends:
        copy.wait()


def shards(*args):
    hbm = pl.BlockSpec(memory_space=pltpu.HBM)
    vmem = pl.BlockSpec(memory_space=pltpu.VMEM)
    smem = pl.BlockSpec(memory_space=pltpu.SMEM)
    operands = list(args)
    operands[5] = operands[5].T
    operands[10] = operands[10].T
    operands = [pltpu.with_memory_space_constraint(a, pltpu.HBM) for a in operands]
    layer_out, gates, kvn = pl.pallas_call(
        layer_kernel,
        out_shape=(
            jax.ShapeDtypeStruct((SEQS, PROPS, FEATS), BF16),
            jax.ShapeDtypeStruct((SEQS, HEADS, PROPS), F32),
            jax.ShapeDtypeStruct((N_KV, PROPS, LANES), BF16),
        ),
        in_specs=[hbm] * len(operands),
        out_specs=(vmem, vmem, vmem),
        scratch_shapes=[
            pltpu.VMEM((SEQS, PROPS, FEATS), BF16),
            pltpu.VMEM((FEATS, 3 * WIDTH), BF16),
            pltpu.VMEM((2 * HEADS, LANES), BF16),
            pltpu.VMEM((2, FEATS, WIDTH), BF16),
            pltpu.VMEM((FEATS,), F32),
            pltpu.VMEM((DH,), F32),
            pltpu.VMEM((DH,), F32),
            pltpu.VMEM((DH,), F32),
            pltpu.VMEM((SEQS, PROPS), jnp.int32),
            pltpu.SMEM((2 * HEADS,), F32),
            pltpu.SMEM((SEQS,), jnp.int32),
            pltpu.SMEM((SEQS,), jnp.int32),
            pltpu.VMEM((SEQS, POS, WIDTH), BF16),
            pltpu.VMEM((SEQS, POS, WIDTH), BF16),
            pltpu.VMEM((SEQS, HEADS, POS), F32),
            pltpu.VMEM((N_KV, 8, LANES), F32),
            pltpu.VMEM((N_KV, 8, LANES), F32),
            pltpu.VMEM((2 * HEADS, 1, LANES), F32),
            pltpu.VMEM((N_KV, 1, LANES), F32),
            pltpu.VMEM((N_KV, PROPS, LANES), BF16),
            pltpu.VMEM((N_KV, PROPS, LANES), BF16),
            pltpu.VMEM((8, LANES), BF16),
            pltpu.VMEM((N_KV, 8, LANES), BF16),
            pltpu.VMEM((PROPS, LANES), BF16),
            pltpu.VMEM((N_KV, PROPS, LANES), BF16),
            pltpu.VMEM((1, LANES), F32),
            pltpu.VMEM((HEADS, 1, LANES), F32),
            pltpu.VMEM((N_KV, 8, LANES), F32),
            pltpu.VMEM((N_KV, 8, LANES), F32),
            pltpu.VMEM((N_KV, 1, LANES), F32),
            pltpu.VMEM((N_KV, 1, LANES), F32),
            pltpu.VMEM((8, LANES), BF16),
            pltpu.VMEM((2 * N_KV, 8, LANES), BF16),
            pltpu.SemaphoreType.DMA((20,)),
            pltpu.SemaphoreType.DMA((24,)),
            pltpu.SemaphoreType.DMA((24,)),
        ],
        compiler_params=pltpu.CompilerParams(
            collective_id=0, has_side_effects=True, vmem_limit_bytes=24 * 2**20
        ),
        name="layer",
    )(*operands)
    key_cache, value_cache, lengths, accepted = args[11], args[12], args[14], args[15]
    layer_out, new_keys, new_values, gates = pl.pallas_call(
        cache_kernel,
        out_shape=(
            jax.ShapeDtypeStruct(layer_out.shape, BF16),
            jax.ShapeDtypeStruct(key_cache.shape, BF16),
            jax.ShapeDtypeStruct(value_cache.shape, BF16),
            jax.ShapeDtypeStruct(gates.shape, F32),
        ),
        in_specs=[vmem, vmem, vmem, smem, smem, vmem, vmem],
        out_specs=(hbm, hbm, hbm, hbm),
        scratch_shapes=[
            pltpu.VMEM((SEQS, POS, WIDTH), BF16),
            pltpu.VMEM((SEQS, POS, WIDTH), BF16),
            pltpu.SemaphoreType.DMA((2 + SEQS,)),
        ],
        compiler_params=pltpu.CompilerParams(vmem_limit_bytes=16 * 2**20),
        name="cache",
    )(key_cache, value_cache, kvn, lengths, accepted, layer_out, gates)
    return layer_out, new_keys, new_values, jnp.transpose(gates, (0, 2, 1))


def solution(mesh):
    placed = (
        P("dp", None, "kv"),
        P("kv"),
        P("kv", "tp"),
        P("kv", "tp"),
        P("kv", "tp"),
        P(),
        P(),
        P(),
        P(),
        P(),
        P("tp", "kv"),
        P("dp", "kv", "tp"),
        P("dp", "kv", "tp"),
        P("dp", "tp", "kv"),
        P("dp"),
        P("dp"),
        P("dp", None),
    )
    return jax.shard_map(
        shards,
        mesh=mesh,
        in_specs=placed,
        out_specs=(
            P("dp", None, "kv"),
            P("dp", "kv", "tp"),
            P("dp", "kv", "tp"),
            P("dp", None, "tp"),
        ),
        check_vma=False,
    )
```

```python
import functools

import jax
import jax.numpy as jnp
from jax import lax
from jax.experimental import pallas as pl
from jax.experimental.pallas import tpu as pltpu
from jax.sharding import PartitionSpec as P

EPSILON = 1e-06
MASKED = -1e30
MESH = pl.DeviceIdType.MESH
F32 = jnp.float32
BF16 = jnp.bfloat16

NZ, NX = 8, 4
N_KV = NZ * NX
SEQS, PROPS, HEADS, DH = 4, 16, 8, 64
ROWS = SEQS * PROPS
WIDTH = HEADS * DH
POS = 512
D = 2048
FEATS = D // N_KV
LANES = 128
FIRST_OWNER = 15341 // POS
CHUNK = 128
QN, GL, KVN, PS, NR, WO, KVZ, TR = 3, 7, 8, 9, 11, 13, 14, 15

OFFSETS = sorted(
    ((dz, dx) for dz in range(NZ) for dx in range(NX) if (dz, dx) != (0, 0)),
    key=lambda o: -(min(o[0], NZ - o[0]) + min(o[1], NX - o[1])),
)


NEAR = [o for o in [(0, 0)] + OFFSETS[::-1] if o[0] in (NZ - 2, NZ - 1, 0, 1)][::-1]
AROUND = [(dz, dx) for dz in (NZ - 2, NZ - 1, 0, 1, 2) for dx in range(NX)]
HALF = N_KV // 2


def iota(shape, dim):
    return lax.broadcasted_iota(jnp.int32, shape, dim)


def swap(x):
    return pltpu.roll(x, DH, 1)


def dot(a, b, dims, precision=None):
    return lax.dot_general(
        a, b, (dims, ((), ())), preferred_element_type=F32, precision=precision
    )


def layer_kernel(
    tokens,
    norm_gain,
    w_query,
    w_key,
    w_value,
    w_forget,
    forget_bias,
    query_gain,
    key_gain,
    head_gain,
    w_out,
    key_cache,
    value_cache,
    gate_cache,
    lengths,
    accepted,
    parents,
    out_ref,
    gates_ref,
    kvn_ref,
    tok_v,
    w_v,
    wf_v,
    wo_v,
    ng_v,
    qg_v,
    kg_v,
    hg_v,
    par_v,
    fb_s,
    len_s,
    acc_s,
    k_v,
    v_v,
    g_v,
    q_send,
    q_recv,
    st_send,
    st_recv,
    kv_send,
    kvx_recv,
    kvz_send,
    kvz_recv,
    qn_send,
    qn_recv,
    kvn_send,
    kvn_recv,
    gl_send,
    gl_recv,
    p_send,
    p_recv,
    ps_send,
    ps_recv,
    t_buf,
    ts_buf,
    n_send,
    n_recv,
    load_sem,
    ssem,
    rsem,
):
    me = lax.axis_index("kv")
    tp = lax.axis_index("tp")
    mz, mx = me // NX, me % NX

    def at(offset):
        return ((mz + offset[0]) % NZ) * NX + (mx + offset[1]) % NX

    peers = [at(o) for o in OFFSETS]
    s_me, h_me = me // HEADS, me % HEADS
    pair, half = me % HALF, me // HALF

    loads = []

    def load(src, dst):
        copy = pltpu.make_async_copy(src, dst, load_sem.at[len(loads)])
        copy.start()
        loads.append(copy)
        return copy

    first = [
        load(tokens, tok_v),
        load(norm_gain, ng_v),
        load(w_query, w_v.at[:, pl.ds(0, WIDTH)]),
        load(w_forget.at[:, pl.ds(pl.multiple_of(me // 2 * LANES, LANES), LANES)], wf_v),
        load(w_key, w_v.at[:, pl.ds(WIDTH, WIDTH)]),
        load(w_value, w_v.at[:, pl.ds(2 * WIDTH, WIDTH)]),
    ]
    barrier = pltpu.get_barrier_semaphore()
    for p in peers:
        pl.semaphore_signal(barrier, inc=1, device_id={"kv": p}, device_id_type=MESH)
    for o in AROUND:
        pl.semaphore_signal(
            barrier, inc=1, device_id={"kv": at(o), "tp": 1 - tp}, device_id_type=MESH
        )
    small = [
        load(parents, par_v),
        load(forget_bias, fb_s),
        load(query_gain, qg_v),
        load(key_gain, kg_v),
        load(head_gain, hg_v),
        load(lengths, len_s),
        load(accepted, acc_s),
    ]
    out_load = load(w_out, wo_v.at[tp])
    cached = [load(key_cache, k_v), load(value_cache, v_v), load(gate_cache, g_v)]

    def send(src, dst, phase, kv, core=None, recv=None):
        pltpu.make_async_remote_copy(
            src_ref=src,
            dst_ref=dst,
            send_sem=ssem.at[phase],
            recv_sem=rsem.at[phase if recv is None else recv],
            device_id={"kv": kv} if core is None else {"kv": kv, "tp": core},
            device_id_type=MESH,
        ).start()

    def await_recv(buf, phase, count):
        part = buf.at[pl.ds(0, count)]
        pltpu.make_async_remote_copy(
            src_ref=part,
            dst_ref=part,
            send_sem=ssem.at[phase],
            recv_sem=rsem.at[phase],
            device_id={"kv": peers[0]},
            device_id_type=MESH,
        ).wait_recv()

    def await_send(buf, phase, count):
        part = buf.at[pl.ds(0, count)]
        pltpu.make_async_remote_copy(
            src_ref=part,
            dst_ref=part,
            send_sem=ssem.at[phase],
            recv_sem=rsem.at[phase],
            device_id={"kv": peers[0]},
            device_id_type=MESH,
        ).wait_send()

    low8 = iota((8, LANES), 1) < DH
    low16 = iota((16, LANES), 1) < DH

    for copy in first:
        copy.wait()
    rows = tok_v[...].reshape(ROWS, FEATS).astype(F32)
    scaled = (rows * ng_v[...].reshape(1, FEATS)).astype(BF16)
    summed = dot(scaled, w_v[...], ((1,), (0,)))
    forget = wf_v[...].astype(F32)
    forget = jnp.where(me % 2 == 1, swap(forget), forget)[:, :FEATS].astype(BF16)
    gate_part = dot(forget, scaled, ((1,), (1,)))
    squares = dot(
        jnp.ones((2 * HEADS, FEATS), F32), rows * rows, ((1,), (1,)), lax.Precision.HIGHEST
    )
    st_send[...] = jnp.concatenate([gate_part, squares], axis=1).reshape(2 * HEADS, 1, LANES)
    for s in range(SEQS):
        for t in range(HEADS // 2):
            a = summed[s * 16 : s * 16 + 8, t * LANES : (t + 1) * LANES]
            b = summed[s * 16 + 8 : s * 16 + 16, t * LANES : (t + 1) * LANES]
            q_send[s * HEADS + 2 * t] = jnp.where(low8, a, swap(b))
            q_send[s * HEADS + 2 * t + 1] = jnp.where(low8, swap(a), b)
    for s in range(SEQS):
        for t in range(HEADS // 2):
            col = WIDTH + t * LANES
            k = summed[s * 16 : s * 16 + 16, col : col + LANES]
            v = summed[s * 16 : s * 16 + 16, col + WIDTH : col + WIDTH + LANES]
            for head, tile in (
                (2 * t, jnp.where(low16, k, swap(v))),
                (2 * t + 1, jnp.where(low16, swap(k), v)),
            ):
                kv_send[head % NX, s * HEADS // NX + head // NX] = tile

    pl.semaphore_wait(barrier, len(OFFSETS) + len(AROUND))

    for p in peers:
        send(q_send.at[p], q_recv.at[me], 0, p)
        send(st_send.at[tp * HEADS + p % HEADS], st_recv.at[me], 1, p)
    for dx in (2, 1, 3):
        other = (mx + dx) % NX
        send(kv_send.at[other], kvx_recv.at[mx], 2, at((0, dx)))
    q_recv[me] = q_send[me]
    st_recv[me] = st_send[tp * HEADS + h_me]

    for copy in small:
        copy.wait()
    out_load.wait()
    send(wo_v.at[tp], wo_v.at[tp], WO, me, 1 - tp)

    parent_row = par_v[pl.ds(s_me, 1), :]
    step_t = (iota((PROPS, PROPS), 0) == parent_row).astype(BF16)
    eye = (iota((PROPS, PROPS), 0) == iota((PROPS, PROPS), 1)).astype(F32)
    ancestors_t = eye + step_t.astype(F32)
    power = step_t
    for _ in range(3):
        power = dot(power, power, ((1,), (0,))).astype(BF16)
        ancestors_t = ancestors_t + dot(ancestors_t.astype(BF16), power, ((1,), (0,)))
    ancestors = ancestors_t.T

    await_recv(st_recv, 1, N_KV - 1)
    stats = jnp.sum(st_recv[...].reshape(N_KV, LANES), axis=0, keepdims=True)
    inverse_row = lax.rsqrt(stats / D + EPSILON)
    logits = stats * swap(inverse_row) + fb_s[tp * HEADS + h_me]
    log_row = jnp.minimum(logits, 0.0) - jnp.log1p(jnp.exp(-jnp.abs(logits)))
    spot = s_me * PROPS
    at_row = iota((PROPS, LANES), 0) + spot
    at_lane = iota((PROPS, LANES), 1)
    inverse = jnp.sum(
        jnp.where(at_lane == at_row + ROWS, inverse_row, 0.0), axis=1, keepdims=True
    )
    own_log = jnp.sum(jnp.where(at_lane == at_row, log_row, 0.0), axis=1, keepdims=True)
    path_row = jnp.sum(ancestors_t * own_log, axis=0, keepdims=True)
    gl_send[...] = log_row

    await_recv(q_recv, 0, N_KV - 1)
    raw = jnp.sum(q_recv[...], axis=0) * jnp.where(low8, inverse[:8], inverse[8:])
    gain = qg_v[...].reshape(1, DH)
    gain = jnp.concatenate([gain, gain], axis=1)
    square = raw * raw
    mean_low = jnp.sum(jnp.where(low8, square, 0.0), axis=1, keepdims=True) / DH
    mean_high = jnp.sum(jnp.where(low8, 0.0, square), axis=1, keepdims=True) / DH
    q_packed = (raw * lax.rsqrt(jnp.where(low8, mean_low, mean_high) + EPSILON) * gain).astype(
        BF16
    )
    qn_send[...] = q_packed

    for p in peers:
        send(qn_send, qn_recv.at[me], QN, p, recv=QN + s_me)
    qn_recv[me] = q_packed

    @pl.when(s_me == 0)
    def _():
        for p in peers:
            send(gl_send, gl_recv.at[h_me], GL, p)
        gl_recv[h_me] = log_row

    await_recv(kvx_recv, 2, NX - 1)
    part = kv_send[mx]
    for dx in (1, 2, 3):
        part = part + kvx_recv[(mx + dx) % NX]
    kvz_send[...] = part
    for dz in (4, 3, 5, 2, 6, 1, 7):
        send(kvz_send.at[(mz + dz) % NZ], kvz_recv.at[mz], KVZ, at((dz, 0)))

    for copy in cached:
        copy.wait()
    pos = iota((1, POS), 1) + me * POS
    diag = iota((PROPS, LANES), 1) - iota((PROPS, LANES), 0)
    corner = (iota((PROPS, LANES), 0) == 0) & (iota((PROPS, LANES), 1) == 2 * PROPS)
    for turn in (0, 1, 3, 2):
        s = (s_me + turn) % SEQS
        await_recv(qn_recv, QN + s, HEADS if turn else HEADS - 1)
        base = len_s[s] + acc_s[s]
        live = pos < base
        gates = g_v[s]
        bound = jnp.sum(jnp.where(pos == base - 1, gates, 0.0), axis=1, keepdims=True)
        for t in range(HEADS // 2):
            m0 = qn_recv[s * HEADS + 2 * t].astype(F32)
            m1 = qn_recv[s * HEADS + 2 * t + 1].astype(F32)
            lhs = jnp.concatenate(
                [
                    jnp.where(low8, m0, 0.0),
                    jnp.where(low8, swap(m0), 0.0),
                    jnp.where(low8, 0.0, swap(m1)),
                    jnp.where(low8, 0.0, m1),
                ],
                axis=0,
            ).astype(BF16)
            keys = k_v[s, :, pl.ds(t * LANES, LANES)]
            values = v_v[s, :, pl.ds(t * LANES, LANES)]
            scores = dot(lhs, keys, ((1,), (1,))) * DH**-0.5
            gate_rows = jnp.concatenate(
                [
                    jnp.broadcast_to(gates[2 * t : 2 * t + 1], (PROPS, POS)),
                    jnp.broadcast_to(gates[2 * t + 1 : 2 * t + 2], (PROPS, POS)),
                ],
                axis=0,
            )
            scores = jnp.where(live, scores - gate_rows, MASKED)
            peak = jnp.max(scores, axis=1, keepdims=True)
            weights = jnp.where(live, jnp.exp(scores - peak), 0.0)
            total = jnp.sum(weights, axis=1, keepdims=True)
            part = dot(weights.astype(BF16), values, ((1,), (0,)))
            at_pair = s % 2 * HEADS + 2 * t
            p_send[at_pair, s // 2] = jnp.where(low8, part[:8], swap(part[8:16])).astype(BF16)
            p_send[at_pair + 1, s // 2] = jnp.where(
                low8, swap(part[16:24]), part[24:32]
            ).astype(BF16)
            for odd in range(2):
                rows_at = slice(odd * PROPS, (odd + 1) * PROPS)
                head = 2 * t + odd
                tile = jnp.where(diag == 0, peak[rows_at], 0.0)
                tile = jnp.where(diag == PROPS, total[rows_at], tile)
                tile = jnp.where(corner, bound[head : head + 1], tile)
                ps_send[s % 2 * HEADS + head, s // 2] = jnp.sum(tile, axis=0, keepdims=True)
        if turn not in (2, 3):
            continue
        for side in (s, (s + 2) % SEQS):
            for j in range(HEADS):
                if turn == 2 and side is not s and j == 0:
                    continue
                head = (h_me + j) % HEADS
                target = side * HEADS + head
                send(p_send.at[s % 2 * HEADS + head], p_recv.at[me], PS, target)
                send(ps_send.at[s % 2 * HEADS + head], ps_recv.at[me], PS + 1, target)
    p_recv[me] = p_send[pair]
    ps_recv[me] = ps_send[pair]

    await_recv(kvz_recv, KVZ, NZ - 1)
    raw_kv = kvz_send[mz]
    for dz in range(1, NZ):
        raw_kv = raw_kv + kvz_recv[(mz + dz) % NZ]
    raw_kv = raw_kv * inverse
    mean_key = jnp.sum(jnp.where(low16, raw_kv * raw_kv, 0.0), axis=1, keepdims=True) / DH
    gain = kg_v[...].reshape(1, DH)
    gain = jnp.concatenate([gain, gain], axis=1)
    kv_new = jnp.where(low16, raw_kv * lax.rsqrt(mean_key + EPSILON) * gain, raw_kv).astype(BF16)
    kvn_send[...] = kv_new
    for owner in range(FIRST_OWNER, N_KV):

        @pl.when(me != owner)
        def _():
            send(kvn_send, kvn_recv.at[me], KVN, owner)

        @pl.when(me == owner)
        def _():
            kvn_recv[me] = kv_new

    q32 = q_packed.astype(F32)
    q_rows = jnp.concatenate(
        [jnp.where(low8, q32, 0.0), jnp.where(low8, swap(q32), 0.0)], axis=0
    ).astype(BF16)
    tree = dot(q_rows, kv_new, ((1,), (1,))) * DH**-0.5 - path_row
    tree_live = ancestors > 0.5
    tree = jnp.where(tree_live, tree, MASKED)
    mirror = (me + HALF) % N_KV
    tree_max = jnp.max(tree, axis=1, keepdims=True)
    tree_weights = jnp.where(tree_live, jnp.exp(tree - tree_max), 0.0)
    tree_total = jnp.sum(tree_weights, axis=1, keepdims=True)
    tree_sum = dot(tree_weights.astype(BF16), kv_new, ((1,), (0,)))
    tree_packed = jnp.where(low8, swap(tree_sum[:8]), tree_sum[8:])
    t_buf[half] = tree_packed
    tile = jnp.where(diag == 0, tree_max, 0.0)
    tile = jnp.where(diag == PROPS, tree_total, tile)
    ts_buf[half] = jnp.sum(tile, axis=0, keepdims=True)
    send(t_buf.at[half], t_buf.at[half], TR, mirror)
    send(ts_buf.at[half], ts_buf.at[half], TR + 1, mirror)

    gain = hg_v[...].reshape(1, DH)
    gain = jnp.concatenate([gain, gain], axis=1)
    await_recv(t_buf, TR, 1)
    await_recv(ts_buf, TR + 1, 1)
    await_recv(ps_recv, PS + 1, N_KV - 1)
    await_recv(p_recv, PS, N_KV - 1)
    for k in range(2):
        stats_t = ps_recv[:, k].reshape(N_KV, LANES).T
        peaks = stats_t[:PROPS]
        bound = jnp.sum(stats_t[2 * PROPS : 2 * PROPS + 1], axis=1, keepdims=True)
        tree_row = ts_buf[k]
        tree_max = jnp.sum(jnp.where(diag == 0, tree_row, 0.0), axis=1, keepdims=True) - bound
        tree_total = jnp.sum(jnp.where(diag == PROPS, tree_row, 0.0), axis=1, keepdims=True)
        top = jnp.maximum(jnp.max(peaks, axis=1, keepdims=True), tree_max)
        factors = jnp.exp(peaks - top)
        tree_factor = jnp.exp(tree_max - top)
        total = (
            jnp.sum(factors * stats_t[PROPS : 2 * PROPS], axis=1, keepdims=True)
            + tree_total * tree_factor
        )
        acc = [t_buf[k] * jnp.where(low8, tree_factor[:8], tree_factor[8:])] + [None] * 3
        for i in range(N_KV):
            factor = jnp.where(low8, factors[:8, i : i + 1], factors[8:, i : i + 1])
            term = p_recv[i, k].astype(F32) * factor
            acc[i % 4] = term if acc[i % 4] is None else acc[i % 4] + term
        weighted = (acc[0] + acc[1]) + (acc[2] + acc[3])
        attended = weighted / jnp.where(low8, total[:8], total[8:])
        square = attended * attended
        mean_low = jnp.sum(jnp.where(low8, square, 0.0), axis=1, keepdims=True) / DH
        mean_high = jnp.sum(jnp.where(low8, 0.0, square), axis=1, keepdims=True) / DH
        n_send[k] = (
            attended * lax.rsqrt(jnp.where(low8, mean_low, mean_high) + EPSILON) * gain
        ).astype(BF16)

    slot = tp * HALF + pair
    for o in NEAR:
        for core in (tp, 1 - tp):
            if o == (0, 0) and core is tp:
                continue
            send(n_send, n_recv.at[slot], NR, at(o), core, recv=NR + s_me % 2)
    n_recv[slot] = n_send[...]

    @pl.when(s_me == 0)
    def _():
        await_recv(gl_recv, GL, HEADS - 1)

    @pl.when(s_me != 0)
    def _():
        await_recv(gl_recv, GL, HEADS)

    logs = gl_recv[...].reshape(HEADS, LANES)
    for s in range(SEQS):
        gates_ref[s] = logs[:, s * PROPS : (s + 1) * PROPS]

    @pl.when(me >= FIRST_OWNER)
    def _():
        await_recv(kvn_recv, KVN, N_KV - 1)
        kvn_ref[...] = kvn_recv[...]

    @pl.when(me < FIRST_OWNER)
    def _():
        kvn_ref[...] = jnp.zeros_like(kvn_ref)

    await_recv(wo_v, WO, 1)
    for turn in (0, 2, 1, 3):
        s = (s_me + turn) % SEQS
        if turn < 2:
            await_recv(n_recv, NR + s % 2, HALF if turn else HALF - 1)
        layer_sum = None
        for core in range(2):
            tiles = []
            for t in range(HEADS // 2):
                spot = core * HALF + s % 2 * HEADS + 2 * t
                m0 = n_recv[spot, s // 2].astype(F32)
                m1 = n_recv[spot + 1, s // 2].astype(F32)
                tiles.append(
                    jnp.concatenate(
                        [jnp.where(low8, m0, swap(m1)), jnp.where(low8, swap(m0), m1)], axis=0
                    ).astype(BF16)
                )
            term = dot(jnp.concatenate(tiles, axis=1), wo_v[core], ((1,), (1,)))
            term = term.astype(BF16).astype(F32)
            layer_sum = term if layer_sum is None else layer_sum + term
        out_ref[s] = layer_sum.astype(BF16)

    await_send(q_send, 0, N_KV - 1)
    await_send(st_recv, 1, N_KV - 1)
    await_send(kvx_recv, 2, NX - 1)
    await_send(kvz_recv, KVZ, NZ - 1)
    await_send(t_buf, TR, 1)
    await_send(ts_buf, TR + 1, 1)
    await_send(qn_recv, QN, N_KV - 1)
    await_send(wo_v, WO, 1)

    @pl.when(s_me == 0)
    def _():
        await_send(st_recv, GL, N_KV - 1)

    @pl.when(me >= FIRST_OWNER)
    def _():
        await_send(kvn_recv, KVN, N_KV - FIRST_OWNER - 1)

    @pl.when(me < FIRST_OWNER)
    def _():
        await_send(kvn_recv, KVN, N_KV - FIRST_OWNER)

    await_send(p_recv, PS, N_KV - 1)
    await_send(ps_recv, PS + 1, N_KV - 1)
    await_send(n_recv, NR, N_KV - 1)


def cache_kernel(
    key_cache,
    value_cache,
    kvn,
    lengths,
    accepted,
    layer_in,
    gates_in,
    layer_out,
    new_keys,
    new_values,
    gates_out,
    k_v,
    v_v,
    sem,
):
    me = lax.axis_index("kv")
    sides = ((key_cache, k_v, new_keys), (value_cache, v_v, new_values))
    ends = [
        pltpu.make_async_copy(layer_in, layer_out, sem.at[0]),
        pltpu.make_async_copy(gates_in, gates_out, sem.at[1]),
    ]

    def write(s, c, side, patched):
        src, buf, dst = sides[side]
        rows = pl.ds(pl.multiple_of(c * CHUNK, CHUNK), CHUNK)
        return pltpu.make_async_copy(
            (buf if patched else src).at[s, rows], dst.at[s, rows], sem.at[2 + s]
        )

    for s in range(SEQS):
        offset = lengths[s] + accepted[s] - me * POS
        for c in range(POS // CHUNK):
            clear = (offset >= (c + 1) * CHUNK) | (offset + PROPS <= c * CHUNK)

            @pl.when(clear)
            def _():
                for side in range(2):
                    write(s, c, side, False).start()

    for copy in ends:
        copy.start()
    low = iota((CHUNK, LANES), 1) < DH

    @pl.when(me >= FIRST_OWNER)
    def _():
        for s in range(SEQS):
            offset = lengths[s] + accepted[s] - me * POS

            def patch(c):
                slot = iota((CHUNK, 1), 0) + c * CHUNK - offset
                hit = (slot >= 0) & (slot < PROPS)
                placing = (slot == iota((CHUNK, PROPS), 1)).astype(BF16)
                rows = pl.ds(pl.multiple_of(c * CHUNK, CHUNK), CHUNK)
                for t in range(HEADS // 2):
                    w0 = dot(placing, kvn[s * HEADS + 2 * t], ((1,), (0,)))
                    w1 = dot(placing, kvn[s * HEADS + 2 * t + 1], ((1,), (0,)))
                    at = (s, rows, pl.ds(t * LANES, LANES))
                    k_v[at] = jnp.where(
                        hit, jnp.where(low, w0, swap(w1)), key_cache[at].astype(F32)
                    ).astype(BF16)
                    v_v[at] = jnp.where(
                        hit, jnp.where(low, swap(w0), w1), value_cache[at].astype(F32)
                    ).astype(BF16)
                for side in range(2):
                    write(s, c, side, True).start()

            first = jnp.maximum(offset, 0) // CHUNK
            last = jnp.minimum(offset + PROPS - 1, POS - 1) // CHUNK

            @pl.when((offset > -PROPS) & (offset < POS))
            def _():
                patch(first)

                @pl.when(last > first)
                def _():
                    patch(last)

    for s in range(SEQS):
        for src, _, dst in sides:
            pltpu.make_async_copy(src.at[s], dst.at[s], sem.at[2 + s]).wait()
    for copy in ends:
        copy.wait()


def shards(*args):
    hbm = pl.BlockSpec(memory_space=pltpu.HBM)
    vmem = pl.BlockSpec(memory_space=pltpu.VMEM)
    smem = pl.BlockSpec(memory_space=pltpu.SMEM)
    operands = list(args)
    operands[5] = operands[5].T
    operands[10] = operands[10].T
    operands = [pltpu.with_memory_space_constraint(a, pltpu.HBM) for a in operands]
    layer_out, gates, kvn = pl.pallas_call(
        layer_kernel,
        out_shape=(
            jax.ShapeDtypeStruct((SEQS, PROPS, FEATS), BF16),
            jax.ShapeDtypeStruct((SEQS, HEADS, PROPS), F32),
            jax.ShapeDtypeStruct((N_KV, PROPS, LANES), BF16),
        ),
        in_specs=[hbm] * len(operands),
        out_specs=(vmem, vmem, vmem),
        scratch_shapes=[
            pltpu.VMEM((SEQS, PROPS, FEATS), BF16),
            pltpu.VMEM((FEATS, 3 * WIDTH), BF16),
            pltpu.VMEM((2 * HEADS, LANES), BF16),
            pltpu.VMEM((2, FEATS, WIDTH), BF16),
            pltpu.VMEM((FEATS,), F32),
            pltpu.VMEM((DH,), F32),
            pltpu.VMEM((DH,), F32),
            pltpu.VMEM((DH,), F32),
            pltpu.VMEM((SEQS, PROPS), jnp.int32),
            pltpu.SMEM((2 * HEADS,), F32),
            pltpu.SMEM((SEQS,), jnp.int32),
            pltpu.SMEM((SEQS,), jnp.int32),
            pltpu.VMEM((SEQS, POS, WIDTH), BF16),
            pltpu.VMEM((SEQS, POS, WIDTH), BF16),
            pltpu.VMEM((SEQS, HEADS, POS), F32),
            pltpu.VMEM((N_KV, 8, LANES), F32),
            pltpu.VMEM((N_KV, 8, LANES), F32),
            pltpu.VMEM((2 * HEADS, 1, LANES), F32),
            pltpu.VMEM((N_KV, 1, LANES), F32),
            pltpu.VMEM((NX, NZ, PROPS, LANES), F32),
            pltpu.VMEM((NX, NZ, PROPS, LANES), F32),
            pltpu.VMEM((NZ, PROPS, LANES), F32),
            pltpu.VMEM((NZ, PROPS, LANES), F32),
            pltpu.VMEM((8, LANES), BF16),
            pltpu.VMEM((N_KV, 8, LANES), BF16),
            pltpu.VMEM((PROPS, LANES), BF16),
            pltpu.VMEM((N_KV, PROPS, LANES), BF16),
            pltpu.VMEM((1, LANES), F32),
            pltpu.VMEM((HEADS, 1, LANES), F32),
            pltpu.VMEM((HALF, 2, 8, LANES), BF16),
            pltpu.VMEM((N_KV, 2, 8, LANES), BF16),
            pltpu.VMEM((HALF, 2, 1, LANES), F32),
            pltpu.VMEM((N_KV, 2, 1, LANES), F32),
            pltpu.VMEM((2, 8, LANES), F32),
            pltpu.VMEM((2, 1, LANES), F32),
            pltpu.VMEM((2, 8, LANES), BF16),
            pltpu.VMEM((2 * HALF, 2, 8, LANES), BF16),
            pltpu.SemaphoreType.DMA((20,)),
            pltpu.SemaphoreType.DMA((24,)),
            pltpu.SemaphoreType.DMA((24,)),
        ],
        compiler_params=pltpu.CompilerParams(
            collective_id=0, has_side_effects=True, vmem_limit_bytes=24 * 2**20
        ),
        name="layer",
    )(*operands)
    key_cache, value_cache, lengths, accepted = args[11], args[12], args[14], args[15]
    layer_out, new_keys, new_values, gates = pl.pallas_call(
        cache_kernel,
        out_shape=(
            jax.ShapeDtypeStruct(layer_out.shape, BF16),
            jax.ShapeDtypeStruct(key_cache.shape, BF16),
            jax.ShapeDtypeStruct(value_cache.shape, BF16),
            jax.ShapeDtypeStruct(gates.shape, F32),
        ),
        in_specs=[vmem, vmem, vmem, smem, smem, vmem, vmem],
        out_specs=(hbm, hbm, hbm, hbm),
        scratch_shapes=[
            pltpu.VMEM((SEQS, POS, WIDTH), BF16),
            pltpu.VMEM((SEQS, POS, WIDTH), BF16),
            pltpu.SemaphoreType.DMA((2 + SEQS,)),
        ],
        compiler_params=pltpu.CompilerParams(vmem_limit_bytes=16 * 2**20),
        name="cache",
    )(key_cache, value_cache, kvn, lengths, accepted, layer_out, gates)
    return layer_out, new_keys, new_values, jnp.transpose(gates, (0, 2, 1))


def solution(mesh):
    placed = (
        P("dp", None, "kv"),
        P("kv"),
        P("kv", "tp"),
        P("kv", "tp"),
        P("kv", "tp"),
        P(),
        P(),
        P(),
        P(),
        P(),
        P("tp", "kv"),
        P("dp", "kv", "tp"),
        P("dp", "kv", "tp"),
        P("dp", "tp", "kv"),
        P("dp"),
        P("dp"),
        P("dp", None),
    )
    return jax.shard_map(
        shards,
        mesh=mesh,
        in_specs=placed,
        out_specs=(
            P("dp", None, "kv"),
            P("dp", "kv", "tp"),
            P("dp", "kv", "tp"),
            P("dp", None, "tp"),
        ),
        check_vma=False,
    )
```

```python
import functools

import jax
import jax.numpy as jnp
from jax import lax
from jax.experimental import pallas as pl
from jax.experimental.pallas import tpu as pltpu
from jax.sharding import PartitionSpec as P

EPSILON = 1e-06
MASKED = -1e30
MESH = pl.DeviceIdType.MESH
F32 = jnp.float32
BF16 = jnp.bfloat16

NZ, NX = 8, 4
N_KV = NZ * NX
SEQS, PROPS, HEADS, DH = 4, 16, 8, 64
ROWS = SEQS * PROPS
WIDTH = HEADS * DH
POS = 512
D = 2048
FEATS = D // N_KV
LANES = 128
FIRST_OWNER = 15341 // POS
EARLY = 2 * NX
CHUNK = 128
QN, GL, KVN, PS, NR, WO, KVZ, TR = 3, 7, 8, 9, 11, 13, 14, 15

OFFSETS = sorted(
    ((dz, dx) for dz in range(NZ) for dx in range(NX) if (dz, dx) != (0, 0)),
    key=lambda o: -(min(o[0], NZ - o[0]) + min(o[1], NX - o[1])),
)


NEAR = [o for o in [(0, 0)] + OFFSETS[::-1] if o[0] in (NZ - 2, NZ - 1, 0, 1)][::-1]
AROUND = [(dz, dx) for dz in (NZ - 2, NZ - 1, 0, 1, 2) for dx in range(NX)]
HALF = N_KV // 2


def iota(shape, dim):
    return lax.broadcasted_iota(jnp.int32, shape, dim)


def swap(x):
    return pltpu.roll(x, DH, 1)


def dot(a, b, dims, precision=None):
    return lax.dot_general(
        a, b, (dims, ((), ())), preferred_element_type=F32, precision=precision
    )


def early_kernel(key_cache, value_cache, new_keys, new_values, token, k_v, v_v, rsem, wsem):
    token[...] = jnp.zeros_like(token)

    @pl.when(lax.axis_index("kv") < EARLY)
    def _():
        reads, writes = [], []
        for s in range(SEQS):
            for i, (src, buf, dst) in enumerate(
                ((key_cache, k_v, new_keys), (value_cache, v_v, new_values))
            ):
                reads.append(pltpu.make_async_copy(src.at[s], buf.at[s], rsem.at[2 * s + i]))
                writes.append(pltpu.make_async_copy(buf.at[s], dst.at[s], wsem.at[2 * s + i]))
        for copy in reads:
            copy.start()
        for read, write in zip(reads, writes):
            read.wait()
            write.start()
        for copy in writes:
            copy.wait()


def layer_kernel(
    tokens,
    norm_gain,
    w_query,
    w_key,
    w_value,
    w_forget,
    forget_bias,
    query_gain,
    key_gain,
    head_gain,
    w_out,
    key_cache,
    value_cache,
    gate_cache,
    lengths,
    accepted,
    parents,
    token,
    out_ref,
    gates_ref,
    kvn_ref,
    tok_v,
    w_v,
    wf_v,
    wo_v,
    ng_v,
    qg_v,
    kg_v,
    hg_v,
    par_v,
    fb_s,
    len_s,
    acc_s,
    k_v,
    v_v,
    g_v,
    q_send,
    q_recv,
    st_send,
    st_recv,
    kv_send,
    kvx_recv,
    kvz_send,
    kvz_recv,
    qn_send,
    qn_recv,
    kvn_send,
    kvn_recv,
    gl_send,
    gl_recv,
    p_send,
    p_recv,
    ps_send,
    ps_recv,
    t_buf,
    ts_buf,
    n_send,
    n_recv,
    load_sem,
    ssem,
    rsem,
):
    me = lax.axis_index("kv")
    tp = lax.axis_index("tp")
    mz, mx = me // NX, me % NX

    def at(offset):
        return ((mz + offset[0]) % NZ) * NX + (mx + offset[1]) % NX

    peers = [at(o) for o in OFFSETS]
    s_me, h_me = me // HEADS, me % HEADS
    pair, half = me % HALF, me // HALF

    loads = []

    def load(src, dst):
        copy = pltpu.make_async_copy(src, dst, load_sem.at[len(loads)])
        copy.start()
        loads.append(copy)
        return copy

    first = [
        load(tokens, tok_v),
        load(norm_gain, ng_v),
        load(w_query, w_v.at[:, pl.ds(0, WIDTH)]),
        load(w_forget.at[:, pl.ds(pl.multiple_of(me // 2 * LANES, LANES), LANES)], wf_v),
        load(w_key, w_v.at[:, pl.ds(WIDTH, WIDTH)]),
        load(w_value, w_v.at[:, pl.ds(2 * WIDTH, WIDTH)]),
    ]
    barrier = pltpu.get_barrier_semaphore()
    for p in peers:
        pl.semaphore_signal(barrier, inc=1, device_id={"kv": p}, device_id_type=MESH)
    for o in AROUND:
        pl.semaphore_signal(
            barrier, inc=1, device_id={"kv": at(o), "tp": 1 - tp}, device_id_type=MESH
        )
    small = [
        load(parents, par_v),
        load(forget_bias, fb_s),
        load(query_gain, qg_v),
        load(key_gain, kg_v),
        load(head_gain, hg_v),
        load(lengths, len_s),
        load(accepted, acc_s),
    ]
    out_load = load(w_out, wo_v.at[tp])
    cached = [load(key_cache, k_v), load(value_cache, v_v), load(gate_cache, g_v)]

    def send(src, dst, phase, kv, core=None, recv=None):
        pltpu.make_async_remote_copy(
            src_ref=src,
            dst_ref=dst,
            send_sem=ssem.at[phase],
            recv_sem=rsem.at[phase if recv is None else recv],
            device_id={"kv": kv} if core is None else {"kv": kv, "tp": core},
            device_id_type=MESH,
        ).start()

    def await_recv(buf, phase, count):
        part = buf.at[pl.ds(0, count)]
        pltpu.make_async_remote_copy(
            src_ref=part,
            dst_ref=part,
            send_sem=ssem.at[phase],
            recv_sem=rsem.at[phase],
            device_id={"kv": peers[0]},
            device_id_type=MESH,
        ).wait_recv()

    def await_send(buf, phase, count):
        part = buf.at[pl.ds(0, count)]
        pltpu.make_async_remote_copy(
            src_ref=part,
            dst_ref=part,
            send_sem=ssem.at[phase],
            recv_sem=rsem.at[phase],
            device_id={"kv": peers[0]},
            device_id_type=MESH,
        ).wait_send()

    low8 = iota((8, LANES), 1) < DH
    low16 = iota((16, LANES), 1) < DH

    for copy in first:
        copy.wait()
    rows = tok_v[...].reshape(ROWS, FEATS).astype(F32)
    scaled = (rows * ng_v[...].reshape(1, FEATS)).astype(BF16)
    summed = dot(scaled, w_v[...], ((1,), (0,)))
    forget = wf_v[...].astype(F32)
    forget = jnp.where(me % 2 == 1, swap(forget), forget)[:, :FEATS].astype(BF16)
    gate_part = dot(forget, scaled, ((1,), (1,)))
    squares = dot(
        jnp.ones((2 * HEADS, FEATS), F32), rows * rows, ((1,), (1,)), lax.Precision.HIGHEST
    )
    st_send[...] = jnp.concatenate([gate_part, squares], axis=1).reshape(2 * HEADS, 1, LANES)
    for s in range(SEQS):
        for t in range(HEADS // 2):
            a = summed[s * 16 : s * 16 + 8, t * LANES : (t + 1) * LANES]
            b = summed[s * 16 + 8 : s * 16 + 16, t * LANES : (t + 1) * LANES]
            q_send[s * HEADS + 2 * t] = jnp.where(low8, a, swap(b))
            q_send[s * HEADS + 2 * t + 1] = jnp.where(low8, swap(a), b)
    for s in range(SEQS):
        for t in range(HEADS // 2):
            col = WIDTH + t * LANES
            k = summed[s * 16 : s * 16 + 16, col : col + LANES]
            v = summed[s * 16 : s * 16 + 16, col + WIDTH : col + WIDTH + LANES]
            for head, tile in (
                (2 * t, jnp.where(low16, k, swap(v))),
                (2 * t + 1, jnp.where(low16, swap(k), v)),
            ):
                kv_send[head % NX, s * HEADS // NX + head // NX] = tile

    pl.semaphore_wait(barrier, len(OFFSETS) + len(AROUND))

    for p in peers:
        send(q_send.at[p], q_recv.at[me], 0, p)
        send(st_send.at[tp * HEADS + p % HEADS], st_recv.at[me], 1, p)
    for dx in (2, 1, 3):
        other = (mx + dx) % NX
        send(kv_send.at[other], kvx_recv.at[mx], 2, at((0, dx)))
    q_recv[me] = q_send[me]
    st_recv[me] = st_send[tp * HEADS + h_me]

    for copy in small:
        copy.wait()
    out_load.wait()
    send(wo_v.at[tp], wo_v.at[tp], WO, me, 1 - tp)

    parent_row = par_v[pl.ds(s_me, 1), :]
    step_t = (iota((PROPS, PROPS), 0) == parent_row).astype(BF16)
    eye = (iota((PROPS, PROPS), 0) == iota((PROPS, PROPS), 1)).astype(F32)
    ancestors_t = eye + step_t.astype(F32)
    power = step_t
    for _ in range(3):
        power = dot(power, power, ((1,), (0,))).astype(BF16)
        ancestors_t = ancestors_t + dot(ancestors_t.astype(BF16), power, ((1,), (0,)))
    ancestors = ancestors_t.T

    await_recv(st_recv, 1, N_KV - 1)
    stats = jnp.sum(st_recv[...].reshape(N_KV, LANES), axis=0, keepdims=True)
    inverse_row = lax.rsqrt(stats / D + EPSILON)
    logits = stats * swap(inverse_row) + fb_s[tp * HEADS + h_me]
    log_row = jnp.minimum(logits, 0.0) - jnp.log1p(jnp.exp(-jnp.abs(logits)))
    spot = s_me * PROPS
    at_row = iota((PROPS, LANES), 0) + spot
    at_lane = iota((PROPS, LANES), 1)
    inverse = jnp.sum(
        jnp.where(at_lane == at_row + ROWS, inverse_row, 0.0), axis=1, keepdims=True
    )
    own_log = jnp.sum(jnp.where(at_lane == at_row, log_row, 0.0), axis=1, keepdims=True)
    path_row = jnp.sum(ancestors_t * own_log, axis=0, keepdims=True)
    gl_send[...] = log_row

    await_recv(q_recv, 0, N_KV - 1)
    raw = jnp.sum(q_recv[...], axis=0) * jnp.where(low8, inverse[:8], inverse[8:])
    gain = qg_v[...].reshape(1, DH)
    gain = jnp.concatenate([gain, gain], axis=1)
    square = raw * raw
    mean_low = jnp.sum(jnp.where(low8, square, 0.0), axis=1, keepdims=True) / DH
    mean_high = jnp.sum(jnp.where(low8, 0.0, square), axis=1, keepdims=True) / DH
    q_packed = (raw * lax.rsqrt(jnp.where(low8, mean_low, mean_high) + EPSILON) * gain).astype(
        BF16
    )
    qn_send[...] = q_packed

    for p in peers:
        send(qn_send, qn_recv.at[me], QN, p, recv=QN + s_me)
    qn_recv[me] = q_packed

    @pl.when(s_me == 0)
    def _():
        for p in peers:
            send(gl_send, gl_recv.at[h_me], GL, p)
        gl_recv[h_me] = log_row

    await_recv(kvx_recv, 2, NX - 1)
    part = kv_send[mx]
    for dx in (1, 2, 3):
        part = part + kvx_recv[(mx + dx) % NX]
    kvz_send[...] = part
    for dz in (4, 3, 5, 2, 6, 1, 7):
        send(kvz_send.at[(mz + dz) % NZ], kvz_recv.at[mz], KVZ, at((dz, 0)))

    for copy in cached:
        copy.wait()
    pos = iota((1, POS), 1) + me * POS
    diag = iota((PROPS, LANES), 1) - iota((PROPS, LANES), 0)
    corner = (iota((PROPS, LANES), 0) == 0) & (iota((PROPS, LANES), 1) == 2 * PROPS)
    for turn in (0, 1, 3, 2):
        s = (s_me + turn) % SEQS
        await_recv(qn_recv, QN + s, HEADS if turn else HEADS - 1)
        base = len_s[s] + acc_s[s]
        live = pos < base
        gates = g_v[s]
        bound = jnp.sum(jnp.where(pos == base - 1, gates, 0.0), axis=1, keepdims=True)
        for t in range(HEADS // 2):
            m0 = qn_recv[s * HEADS + 2 * t].astype(F32)
            m1 = qn_recv[s * HEADS + 2 * t + 1].astype(F32)
            lhs = jnp.concatenate(
                [
                    jnp.where(low8, m0, 0.0),
                    jnp.where(low8, swap(m0), 0.0),
                    jnp.where(low8, 0.0, swap(m1)),
                    jnp.where(low8, 0.0, m1),
                ],
                axis=0,
            ).astype(BF16)
            keys = k_v[s, :, pl.ds(t * LANES, LANES)]
            values = v_v[s, :, pl.ds(t * LANES, LANES)]
            scores = dot(lhs, keys, ((1,), (1,))) * DH**-0.5
            gate_rows = jnp.concatenate(
                [
                    jnp.broadcast_to(gates[2 * t : 2 * t + 1], (PROPS, POS)),
                    jnp.broadcast_to(gates[2 * t + 1 : 2 * t + 2], (PROPS, POS)),
                ],
                axis=0,
            )
            scores = jnp.where(live, scores - gate_rows, MASKED)
            peak = jnp.max(scores, axis=1, keepdims=True)
            weights = jnp.where(live, jnp.exp(scores - peak), 0.0)
            total = jnp.sum(weights, axis=1, keepdims=True)
            part = dot(weights.astype(BF16), values, ((1,), (0,)))
            at_pair = s % 2 * HEADS + 2 * t
            p_send[at_pair, s // 2] = jnp.where(low8, part[:8], swap(part[8:16])).astype(BF16)
            p_send[at_pair + 1, s // 2] = jnp.where(
                low8, swap(part[16:24]), part[24:32]
            ).astype(BF16)
            for odd in range(2):
                rows_at = slice(odd * PROPS, (odd + 1) * PROPS)
                head = 2 * t + odd
                tile = jnp.where(diag == 0, peak[rows_at], 0.0)
                tile = jnp.where(diag == PROPS, total[rows_at], tile)
                tile = jnp.where(corner, bound[head : head + 1], tile)
                ps_send[s % 2 * HEADS + head, s // 2] = jnp.sum(tile, axis=0, keepdims=True)
        if turn not in (2, 3):
            continue
        for side in (s, (s + 2) % SEQS):
            for j in range(HEADS):
                if turn == 2 and side is not s and j == 0:
                    continue
                head = (h_me + j) % HEADS
                target = side * HEADS + head
                send(p_send.at[s % 2 * HEADS + head], p_recv.at[me], PS, target)
                send(ps_send.at[s % 2 * HEADS + head], ps_recv.at[me], PS + 1, target)
    p_recv[me] = p_send[pair]
    ps_recv[me] = ps_send[pair]

    await_recv(kvz_recv, KVZ, NZ - 1)
    raw_kv = kvz_send[mz]
    for dz in range(1, NZ):
        raw_kv = raw_kv + kvz_recv[(mz + dz) % NZ]
    raw_kv = raw_kv * inverse
    mean_key = jnp.sum(jnp.where(low16, raw_kv * raw_kv, 0.0), axis=1, keepdims=True) / DH
    gain = kg_v[...].reshape(1, DH)
    gain = jnp.concatenate([gain, gain], axis=1)
    kv_new = jnp.where(low16, raw_kv * lax.rsqrt(mean_key + EPSILON) * gain, raw_kv).astype(BF16)
    kvn_send[...] = kv_new
    for owner in range(FIRST_OWNER, N_KV):

        @pl.when(me != owner)
        def _():
            send(kvn_send, kvn_recv.at[me], KVN, owner)

        @pl.when(me == owner)
        def _():
            kvn_recv[me] = kv_new

    q32 = q_packed.astype(F32)
    q_rows = jnp.concatenate(
        [jnp.where(low8, q32, 0.0), jnp.where(low8, swap(q32), 0.0)], axis=0
    ).astype(BF16)
    tree = dot(q_rows, kv_new, ((1,), (1,))) * DH**-0.5 - path_row
    tree_live = ancestors > 0.5
    tree = jnp.where(tree_live, tree, MASKED)
    mirror = (me + HALF) % N_KV
    tree_max = jnp.max(tree, axis=1, keepdims=True)
    tree_weights = jnp.where(tree_live, jnp.exp(tree - tree_max), 0.0)
    tree_total = jnp.sum(tree_weights, axis=1, keepdims=True)
    tree_sum = dot(tree_weights.astype(BF16), kv_new, ((1,), (0,)))
    tree_packed = jnp.where(low8, swap(tree_sum[:8]), tree_sum[8:])
    t_buf[half] = tree_packed
    tile = jnp.where(diag == 0, tree_max, 0.0)
    tile = jnp.where(diag == PROPS, tree_total, tile)
    ts_buf[half] = jnp.sum(tile, axis=0, keepdims=True)
    send(t_buf.at[half], t_buf.at[half], TR, mirror)
    send(ts_buf.at[half], ts_buf.at[half], TR + 1, mirror)

    gain = hg_v[...].reshape(1, DH)
    gain = jnp.concatenate([gain, gain], axis=1)
    await_recv(t_buf, TR, 1)
    await_recv(ts_buf, TR + 1, 1)
    await_recv(ps_recv, PS + 1, N_KV - 1)
    await_recv(p_recv, PS, N_KV - 1)
    for k in range(2):
        stats_t = ps_recv[:, k].reshape(N_KV, LANES).T
        peaks = stats_t[:PROPS]
        bound = jnp.sum(stats_t[2 * PROPS : 2 * PROPS + 1], axis=1, keepdims=True)
        tree_row = ts_buf[k]
        tree_max = jnp.sum(jnp.where(diag == 0, tree_row, 0.0), axis=1, keepdims=True) - bound
        tree_total = jnp.sum(jnp.where(diag == PROPS, tree_row, 0.0), axis=1, keepdims=True)
        top = jnp.maximum(jnp.max(peaks, axis=1, keepdims=True), tree_max)
        factors = jnp.exp(peaks - top)
        tree_factor = jnp.exp(tree_max - top)
        total = (
            jnp.sum(factors * stats_t[PROPS : 2 * PROPS], axis=1, keepdims=True)
            + tree_total * tree_factor
        )
        acc = [t_buf[k] * jnp.where(low8, tree_factor[:8], tree_factor[8:])] + [None] * 3
        for i in range(N_KV):
            factor = jnp.where(low8, factors[:8, i : i + 1], factors[8:, i : i + 1])
            term = p_recv[i, k].astype(F32) * factor
            acc[i % 4] = term if acc[i % 4] is None else acc[i % 4] + term
        weighted = (acc[0] + acc[1]) + (acc[2] + acc[3])
        attended = weighted / jnp.where(low8, total[:8], total[8:])
        square = attended * attended
        mean_low = jnp.sum(jnp.where(low8, square, 0.0), axis=1, keepdims=True) / DH
        mean_high = jnp.sum(jnp.where(low8, 0.0, square), axis=1, keepdims=True) / DH
        n_send[k] = (
            attended * lax.rsqrt(jnp.where(low8, mean_low, mean_high) + EPSILON) * gain
        ).astype(BF16)

    slot = tp * HALF + pair
    for o in NEAR:
        for core in (tp, 1 - tp):
            if o == (0, 0) and core is tp:
                continue
            send(n_send, n_recv.at[slot], NR, at(o), core, recv=NR + s_me % 2)
    n_recv[slot] = n_send[...]

    @pl.when(s_me == 0)
    def _():
        await_recv(gl_recv, GL, HEADS - 1)

    @pl.when(s_me != 0)
    def _():
        await_recv(gl_recv, GL, HEADS)

    logs = gl_recv[...].reshape(HEADS, LANES)
    for s in range(SEQS):
        gates_ref[s] = logs[:, s * PROPS : (s + 1) * PROPS]

    @pl.when(me >= FIRST_OWNER)
    def _():
        await_recv(kvn_recv, KVN, N_KV - 1)
        kvn_ref[...] = kvn_recv[...]

    @pl.when(me < FIRST_OWNER)
    def _():
        kvn_ref[...] = jnp.zeros_like(kvn_ref)

    await_recv(wo_v, WO, 1)
    for turn in (0, 2, 1, 3):
        s = (s_me + turn) % SEQS
        if turn < 2:
            await_recv(n_recv, NR + s % 2, HALF if turn else HALF - 1)
        layer_sum = None
        for core in range(2):
            tiles = []
            for t in range(HEADS // 2):
                spot = core * HALF + s % 2 * HEADS + 2 * t
                m0 = n_recv[spot, s // 2].astype(F32)
                m1 = n_recv[spot + 1, s // 2].astype(F32)
                tiles.append(
                    jnp.concatenate(
                        [jnp.where(low8, m0, swap(m1)), jnp.where(low8, swap(m0), m1)], axis=0
                    ).astype(BF16)
                )
            term = dot(jnp.concatenate(tiles, axis=1), wo_v[core], ((1,), (1,)))
            term = term.astype(BF16).astype(F32)
            layer_sum = term if layer_sum is None else layer_sum + term
        out_ref[s] = layer_sum.astype(BF16)

    await_send(q_send, 0, N_KV - 1)
    await_send(st_recv, 1, N_KV - 1)
    await_send(kvx_recv, 2, NX - 1)
    await_send(kvz_recv, KVZ, NZ - 1)
    await_send(t_buf, TR, 1)
    await_send(ts_buf, TR + 1, 1)
    await_send(qn_recv, QN, N_KV - 1)
    await_send(wo_v, WO, 1)

    @pl.when(s_me == 0)
    def _():
        await_send(st_recv, GL, N_KV - 1)

    @pl.when(me >= FIRST_OWNER)
    def _():
        await_send(kvn_recv, KVN, N_KV - FIRST_OWNER - 1)

    @pl.when(me < FIRST_OWNER)
    def _():
        await_send(kvn_recv, KVN, N_KV - FIRST_OWNER)

    await_send(p_recv, PS, N_KV - 1)
    await_send(ps_recv, PS + 1, N_KV - 1)
    await_send(n_recv, NR, N_KV - 1)


def cache_kernel(
    key_cache,
    value_cache,
    kvn,
    lengths_in,
    accepted_in,
    layer_in,
    gates_in,
    keys_in,
    values_in,
    layer_out,
    new_keys,
    new_values,
    gates_out,
    k_v,
    v_v,
    lengths,
    accepted,
    sem,
    small_sem,
):
    me = lax.axis_index("kv")
    sides = ((key_cache, k_v, new_keys), (value_cache, v_v, new_values))
    ends = [
        pltpu.make_async_copy(layer_in, layer_out, sem.at[0]),
        pltpu.make_async_copy(gates_in, gates_out, sem.at[1]),
    ]
    for copy in ends:
        copy.start()

    def write(s, c, side, patched):
        src, buf, dst = sides[side]
        rows = pl.ds(pl.multiple_of(c * CHUNK, CHUNK), CHUNK)
        return pltpu.make_async_copy(
            (buf if patched else src).at[s, rows], dst.at[s, rows], sem.at[2 + s]
        )

    def whole(s, src, dst):
        return pltpu.make_async_copy(src.at[s], dst.at[s], sem.at[2 + s])

    @pl.when((me >= EARLY) & (me < FIRST_OWNER))
    def _():
        for s in range(SEQS):
            for src, _, dst in sides:
                whole(s, src, dst).start()

    low = iota((CHUNK, LANES), 1) < DH

    @pl.when(me >= FIRST_OWNER)
    def _():
        small = [
            pltpu.make_async_copy(lengths_in, lengths, small_sem.at[0]),
            pltpu.make_async_copy(accepted_in, accepted, small_sem.at[1]),
        ]
        for copy in small:
            copy.start()
        for copy in small:
            copy.wait()
        for s in range(SEQS):
            offset = lengths[s] + accepted[s] - me * POS
            for c in range(POS // CHUNK):
                clear = (offset >= (c + 1) * CHUNK) | (offset + PROPS <= c * CHUNK)

                @pl.when(clear)
                def _():
                    for side in range(2):
                        write(s, c, side, False).start()

        for s in range(SEQS):
            offset = lengths[s] + accepted[s] - me * POS

            def patch(c):
                slot = iota((CHUNK, 1), 0) + c * CHUNK - offset
                hit = (slot >= 0) & (slot < PROPS)
                placing = (slot == iota((CHUNK, PROPS), 1)).astype(BF16)
                rows = pl.ds(pl.multiple_of(c * CHUNK, CHUNK), CHUNK)
                for t in range(HEADS // 2):
                    w0 = dot(placing, kvn[s * HEADS + 2 * t], ((1,), (0,)))
                    w1 = dot(placing, kvn[s * HEADS + 2 * t + 1], ((1,), (0,)))
                    at = (s, rows, pl.ds(t * LANES, LANES))
                    k_v[at] = jnp.where(
                        hit, jnp.where(low, w0, swap(w1)), key_cache[at].astype(F32)
                    ).astype(BF16)
                    v_v[at] = jnp.where(
                        hit, jnp.where(low, swap(w0), w1), value_cache[at].astype(F32)
                    ).astype(BF16)
                for side in range(2):
                    write(s, c, side, True).start()

            first = jnp.maximum(offset, 0) // CHUNK
            last = jnp.minimum(offset + PROPS - 1, POS - 1) // CHUNK

            @pl.when((offset > -PROPS) & (offset < POS))
            def _():
                patch(first)

                @pl.when(last > first)
                def _():
                    patch(last)

    @pl.when(me >= EARLY)
    def _():
        for s in range(SEQS):
            for src, _, dst in sides:
                whole(s, src, dst).wait()

    for copy in ends:
        copy.wait()


def shards(*args):
    hbm = pl.BlockSpec(memory_space=pltpu.HBM)
    vmem = pl.BlockSpec(memory_space=pltpu.VMEM)
    operands = list(args)
    operands[5] = operands[5].T
    operands[10] = operands[10].T
    operands = [pltpu.with_memory_space_constraint(a, pltpu.HBM) for a in operands]
    key_cache, value_cache = args[11], args[12]
    early_keys, early_values, token = pl.pallas_call(
        early_kernel,
        out_shape=(
            jax.ShapeDtypeStruct(key_cache.shape, BF16),
            jax.ShapeDtypeStruct(value_cache.shape, BF16),
            jax.ShapeDtypeStruct((8, LANES), F32),
        ),
        in_specs=[hbm, hbm],
        out_specs=(hbm, hbm, vmem),
        scratch_shapes=[
            pltpu.VMEM((SEQS, POS, WIDTH), BF16),
            pltpu.VMEM((SEQS, POS, WIDTH), BF16),
            pltpu.SemaphoreType.DMA((2 * SEQS,)),
            pltpu.SemaphoreType.DMA((2 * SEQS,)),
        ],
        compiler_params=pltpu.CompilerParams(vmem_limit_bytes=16 * 2**20),
        name="early",
    )(operands[11], operands[12])
    layer_out, gates, kvn = pl.pallas_call(
        layer_kernel,
        out_shape=(
            jax.ShapeDtypeStruct((SEQS, PROPS, FEATS), BF16),
            jax.ShapeDtypeStruct((SEQS, HEADS, PROPS), F32),
            jax.ShapeDtypeStruct((N_KV, PROPS, LANES), BF16),
        ),
        in_specs=[hbm] * len(operands) + [pl.BlockSpec(memory_space=pl.ANY)],
        out_specs=(vmem, vmem, vmem),
        scratch_shapes=[
            pltpu.VMEM((SEQS, PROPS, FEATS), BF16),
            pltpu.VMEM((FEATS, 3 * WIDTH), BF16),
            pltpu.VMEM((2 * HEADS, LANES), BF16),
            pltpu.VMEM((2, FEATS, WIDTH), BF16),
            pltpu.VMEM((FEATS,), F32),
            pltpu.VMEM((DH,), F32),
            pltpu.VMEM((DH,), F32),
            pltpu.VMEM((DH,), F32),
            pltpu.VMEM((SEQS, PROPS), jnp.int32),
            pltpu.SMEM((2 * HEADS,), F32),
            pltpu.SMEM((SEQS,), jnp.int32),
            pltpu.SMEM((SEQS,), jnp.int32),
            pltpu.VMEM((SEQS, POS, WIDTH), BF16),
            pltpu.VMEM((SEQS, POS, WIDTH), BF16),
            pltpu.VMEM((SEQS, HEADS, POS), F32),
            pltpu.VMEM((N_KV, 8, LANES), F32),
            pltpu.VMEM((N_KV, 8, LANES), F32),
            pltpu.VMEM((2 * HEADS, 1, LANES), F32),
            pltpu.VMEM((N_KV, 1, LANES), F32),
            pltpu.VMEM((NX, NZ, PROPS, LANES), F32),
            pltpu.VMEM((NX, NZ, PROPS, LANES), F32),
            pltpu.VMEM((NZ, PROPS, LANES), F32),
            pltpu.VMEM((NZ, PROPS, LANES), F32),
            pltpu.VMEM((8, LANES), BF16),
            pltpu.VMEM((N_KV, 8, LANES), BF16),
            pltpu.VMEM((PROPS, LANES), BF16),
            pltpu.VMEM((N_KV, PROPS, LANES), BF16),
            pltpu.VMEM((1, LANES), F32),
            pltpu.VMEM((HEADS, 1, LANES), F32),
            pltpu.VMEM((HALF, 2, 8, LANES), BF16),
            pltpu.VMEM((N_KV, 2, 8, LANES), BF16),
            pltpu.VMEM((HALF, 2, 1, LANES), F32),
            pltpu.VMEM((N_KV, 2, 1, LANES), F32),
            pltpu.VMEM((2, 8, LANES), F32),
            pltpu.VMEM((2, 1, LANES), F32),
            pltpu.VMEM((2, 8, LANES), BF16),
            pltpu.VMEM((2 * HALF, 2, 8, LANES), BF16),
            pltpu.SemaphoreType.DMA((20,)),
            pltpu.SemaphoreType.DMA((24,)),
            pltpu.SemaphoreType.DMA((24,)),
        ],
        compiler_params=pltpu.CompilerParams(
            collective_id=0, has_side_effects=True, vmem_limit_bytes=24 * 2**20
        ),
        name="layer",
    )(*operands, token)
    layer_out, new_keys, new_values, gates = pl.pallas_call(
        cache_kernel,
        out_shape=(
            jax.ShapeDtypeStruct(layer_out.shape, BF16),
            jax.ShapeDtypeStruct(key_cache.shape, BF16),
            jax.ShapeDtypeStruct(value_cache.shape, BF16),
            jax.ShapeDtypeStruct(gates.shape, F32),
        ),
        in_specs=[vmem, vmem, vmem, hbm, hbm, vmem, vmem, hbm, hbm],
        out_specs=(hbm, hbm, hbm, hbm),
        input_output_aliases={7: 1, 8: 2},
        scratch_shapes=[
            pltpu.VMEM((SEQS, POS, WIDTH), BF16),
            pltpu.VMEM((SEQS, POS, WIDTH), BF16),
            pltpu.SMEM((SEQS,), jnp.int32),
            pltpu.SMEM((SEQS,), jnp.int32),
            pltpu.SemaphoreType.DMA((2 + SEQS,)),
            pltpu.SemaphoreType.DMA((2,)),
        ],
        compiler_params=pltpu.CompilerParams(vmem_limit_bytes=16 * 2**20),
        name="cache",
    )(
        key_cache,
        value_cache,
        kvn,
        operands[14],
        operands[15],
        layer_out,
        gates,
        early_keys,
        early_values,
    )
    return layer_out, new_keys, new_values, jnp.transpose(gates, (0, 2, 1))


def solution(mesh):
    placed = (
        P("dp", None, "kv"),
        P("kv"),
        P("kv", "tp"),
        P("kv", "tp"),
        P("kv", "tp"),
        P(),
        P(),
        P(),
        P(),
        P(),
        P("tp", "kv"),
        P("dp", "kv", "tp"),
        P("dp", "kv", "tp"),
        P("dp", "tp", "kv"),
        P("dp"),
        P("dp"),
        P("dp", None),
    )
    return jax.shard_map(
        shards,
        mesh=mesh,
        in_specs=placed,
        out_specs=(
            P("dp", None, "kv"),
            P("dp", "kv", "tp"),
            P("dp", "kv", "tp"),
            P("dp", None, "tp"),
        ),
        check_vma=False,
    )
```

```python
import functools

import jax
import jax.numpy as jnp
from jax import lax
from jax.experimental import pallas as pl
from jax.experimental.pallas import tpu as pltpu
from jax.sharding import PartitionSpec as P

EPSILON = 1e-06
MASKED = -1e30
MESH = pl.DeviceIdType.MESH
F32 = jnp.float32
BF16 = jnp.bfloat16

NZ, NX = 8, 4
N_KV = NZ * NX
SEQS, PROPS, HEADS, DH = 4, 16, 8, 64
ROWS = SEQS * PROPS
WIDTH = HEADS * DH
POS = 512
D = 2048
FEATS = D // N_KV
LANES = 128
FIRST_OWNER = 15341 // POS
EARLY = 2 * NX
CHUNK = 128
QN, GL, KVN, PS, NR, WO, KVZ, TR = 3, 7, 8, 9, 11, 13, 14, 15

OFFSETS = sorted(
    ((dz, dx) for dz in range(NZ) for dx in range(NX) if (dz, dx) != (0, 0)),
    key=lambda o: -(min(o[0], NZ - o[0]) + min(o[1], NX - o[1])),
)


NEAR = [o for o in [(0, 0)] + OFFSETS[::-1] if o[0] in (NZ - 2, NZ - 1, 0, 1)][::-1]
AROUND = [(dz, dx) for dz in (NZ - 2, NZ - 1, 0, 1, 2) for dx in range(NX)]
HALF = N_KV // 2


def iota(shape, dim):
    return lax.broadcasted_iota(jnp.int32, shape, dim)


def swap(x):
    return pltpu.roll(x, DH, 1)


def dot(a, b, dims, precision=None):
    return lax.dot_general(
        a, b, (dims, ((), ())), preferred_element_type=F32, precision=precision
    )


def early_kernel(key_cache, value_cache, new_keys, new_values, token, k_v, v_v, rsem, wsem):
    token[...] = jnp.zeros_like(token)

    @pl.when(lax.axis_index("kv") < EARLY)
    def _():
        reads, writes = [], []
        for s in range(SEQS):
            for i, (src, buf, dst) in enumerate(
                ((key_cache, k_v, new_keys), (value_cache, v_v, new_values))
            ):
                reads.append(pltpu.make_async_copy(src.at[s], buf.at[s], rsem.at[2 * s + i]))
                writes.append(pltpu.make_async_copy(buf.at[s], dst.at[s], wsem.at[2 * s + i]))
        for copy in reads:
            copy.start()
        for read, write in zip(reads, writes):
            read.wait()
            write.start()
        for copy in writes:
            copy.wait()


def layer_kernel(
    tokens,
    norm_gain,
    w_query,
    w_key,
    w_value,
    w_forget,
    forget_bias,
    query_gain,
    key_gain,
    head_gain,
    w_out,
    key_cache,
    value_cache,
    gate_cache,
    lengths,
    accepted,
    parents,
    token,
    out_ref,
    gates_ref,
    kvn_ref,
    tok_v,
    w_v,
    wf_v,
    wo_v,
    ng_v,
    qg_v,
    kg_v,
    hg_v,
    par_v,
    fb_s,
    len_s,
    acc_s,
    k_v,
    v_v,
    g_v,
    q_send,
    q_recv,
    st_send,
    st_recv,
    kv_send,
    kvx_recv,
    kvz_send,
    kvz_recv,
    qn_send,
    qn_recv,
    kvn_send,
    kvn_recv,
    gl_send,
    gl_recv,
    p_send,
    p_recv,
    ps_send,
    ps_recv,
    t_buf,
    ts_buf,
    n_send,
    n_recv,
    t_send,
    ts_send,
    load_sem,
    ssem,
    rsem,
):
    me = lax.axis_index("kv")
    tp = lax.axis_index("tp")
    mz, mx = me // NX, me % NX

    def at(offset):
        return ((mz + offset[0]) % NZ) * NX + (mx + offset[1]) % NX

    peers = [at(o) for o in OFFSETS]
    s_me, h_me = me // HEADS, me % HEADS
    half = me // HALF
    pair = (mz + 2) % (NZ // 2) * NX + (mx + NX - 1) % NX
    group = pair // HEADS
    other_half = (me + HALF) % N_KV

    loads = []

    def load(src, dst):
        copy = pltpu.make_async_copy(src, dst, load_sem.at[len(loads)])
        copy.start()
        loads.append(copy)
        return copy

    first = [
        load(tokens, tok_v),
        load(norm_gain, ng_v),
        load(w_query, w_v.at[:, pl.ds(0, WIDTH)]),
        load(w_forget.at[:, pl.ds(pl.multiple_of(me // 2 * LANES, LANES), LANES)], wf_v),
        load(w_key, w_v.at[:, pl.ds(WIDTH, WIDTH)]),
        load(w_value, w_v.at[:, pl.ds(2 * WIDTH, WIDTH)]),
    ]
    barrier = pltpu.get_barrier_semaphore()
    for p in peers:
        pl.semaphore_signal(barrier, inc=1, device_id={"kv": p}, device_id_type=MESH)
    for o in AROUND:
        pl.semaphore_signal(
            barrier, inc=1, device_id={"kv": at(o), "tp": 1 - tp}, device_id_type=MESH
        )
    small = [
        load(parents, par_v),
        load(forget_bias, fb_s),
        load(query_gain, qg_v),
        load(key_gain, kg_v),
        load(head_gain, hg_v),
        load(lengths, len_s),
        load(accepted, acc_s),
    ]
    out_load = load(w_out, wo_v.at[tp])
    cached = [load(key_cache, k_v), load(value_cache, v_v), load(gate_cache, g_v)]

    def send(src, dst, phase, kv, core=None, recv=None):
        pltpu.make_async_remote_copy(
            src_ref=src,
            dst_ref=dst,
            send_sem=ssem.at[phase],
            recv_sem=rsem.at[phase if recv is None else recv],
            device_id={"kv": kv} if core is None else {"kv": kv, "tp": core},
            device_id_type=MESH,
        ).start()

    def await_recv(buf, phase, count):
        part = buf.at[pl.ds(0, count)]
        pltpu.make_async_remote_copy(
            src_ref=part,
            dst_ref=part,
            send_sem=ssem.at[phase],
            recv_sem=rsem.at[phase],
            device_id={"kv": peers[0]},
            device_id_type=MESH,
        ).wait_recv()

    def await_send(buf, phase, count):
        part = buf.at[pl.ds(0, count)]
        pltpu.make_async_remote_copy(
            src_ref=part,
            dst_ref=part,
            send_sem=ssem.at[phase],
            recv_sem=rsem.at[phase],
            device_id={"kv": peers[0]},
            device_id_type=MESH,
        ).wait_send()

    low8 = iota((8, LANES), 1) < DH
    low16 = iota((16, LANES), 1) < DH

    for copy in first:
        copy.wait()
    rows = tok_v[...].reshape(ROWS, FEATS).astype(F32)
    scaled = (rows * ng_v[...].reshape(1, FEATS)).astype(BF16)
    summed = dot(scaled, w_v[...], ((1,), (0,)))
    forget = wf_v[...].astype(F32)
    forget = jnp.where(me % 2 == 1, swap(forget), forget)[:, :FEATS].astype(BF16)
    gate_part = dot(forget, scaled, ((1,), (1,)))
    squares = dot(
        jnp.ones((2 * HEADS, FEATS), F32), rows * rows, ((1,), (1,)), lax.Precision.HIGHEST
    )
    st_send[...] = jnp.concatenate([gate_part, squares], axis=1).reshape(2 * HEADS, 1, LANES)
    for s in range(SEQS):
        for t in range(HEADS // 2):
            a = summed[s * 16 : s * 16 + 8, t * LANES : (t + 1) * LANES]
            b = summed[s * 16 + 8 : s * 16 + 16, t * LANES : (t + 1) * LANES]
            q_send[s * HEADS + 2 * t] = jnp.where(low8, a, swap(b))
            q_send[s * HEADS + 2 * t + 1] = jnp.where(low8, swap(a), b)
    for s in range(SEQS):
        for t in range(HEADS // 2):
            col = WIDTH + t * LANES
            k = summed[s * 16 : s * 16 + 16, col : col + LANES]
            v = summed[s * 16 : s * 16 + 16, col + WIDTH : col + WIDTH + LANES]
            for head, tile in (
                (2 * t, jnp.where(low16, k, swap(v))),
                (2 * t + 1, jnp.where(low16, swap(k), v)),
            ):
                kv_send[head % NX, s * HEADS // NX + head // NX] = tile

    pl.semaphore_wait(barrier, len(OFFSETS) + len(AROUND))

    for p in peers:
        send(q_send.at[p], q_recv.at[me], 0, p)
        send(st_send.at[tp * HEADS + p % HEADS], st_recv.at[me], 1, p)
    for dx in (2, 1, 3):
        other = (mx + dx) % NX
        send(kv_send.at[other], kvx_recv.at[mx], 2, at((0, dx)))
    q_recv[me] = q_send[me]
    st_recv[me] = st_send[tp * HEADS + h_me]

    for copy in small:
        copy.wait()
    out_load.wait()
    send(wo_v.at[tp], wo_v.at[tp], WO, me, 1 - tp)

    parent_row = par_v[pl.ds(s_me, 1), :]
    step_t = (iota((PROPS, PROPS), 0) == parent_row).astype(BF16)
    eye = (iota((PROPS, PROPS), 0) == iota((PROPS, PROPS), 1)).astype(F32)
    ancestors_t = eye + step_t.astype(F32)
    power = step_t
    for _ in range(3):
        power = dot(power, power, ((1,), (0,))).astype(BF16)
        ancestors_t = ancestors_t + dot(ancestors_t.astype(BF16), power, ((1,), (0,)))
    ancestors = ancestors_t.T

    await_recv(st_recv, 1, N_KV - 1)
    stats = jnp.sum(st_recv[...].reshape(N_KV, LANES), axis=0, keepdims=True)
    inverse_row = lax.rsqrt(stats / D + EPSILON)
    logits = stats * swap(inverse_row) + fb_s[tp * HEADS + h_me]
    log_row = jnp.minimum(logits, 0.0) - jnp.log1p(jnp.exp(-jnp.abs(logits)))
    spot = s_me * PROPS
    at_row = iota((PROPS, LANES), 0) + spot
    at_lane = iota((PROPS, LANES), 1)
    inverse = jnp.sum(
        jnp.where(at_lane == at_row + ROWS, inverse_row, 0.0), axis=1, keepdims=True
    )
    own_log = jnp.sum(jnp.where(at_lane == at_row, log_row, 0.0), axis=1, keepdims=True)
    path_row = jnp.sum(ancestors_t * own_log, axis=0, keepdims=True)
    gl_send[...] = log_row

    await_recv(q_recv, 0, N_KV - 1)
    raw = jnp.sum(q_recv[...], axis=0) * jnp.where(low8, inverse[:8], inverse[8:])
    gain = qg_v[...].reshape(1, DH)
    gain = jnp.concatenate([gain, gain], axis=1)
    square = raw * raw
    mean_low = jnp.sum(jnp.where(low8, square, 0.0), axis=1, keepdims=True) / DH
    mean_high = jnp.sum(jnp.where(low8, 0.0, square), axis=1, keepdims=True) / DH
    q_packed = (raw * lax.rsqrt(jnp.where(low8, mean_low, mean_high) + EPSILON) * gain).astype(
        BF16
    )
    qn_send[...] = q_packed

    for p in peers:
        send(qn_send, qn_recv.at[me], QN, p, recv=QN + s_me)
    qn_recv[me] = q_packed

    @pl.when(s_me == 0)
    def _():
        for p in peers:
            send(gl_send, gl_recv.at[h_me], GL, p)
        gl_recv[h_me] = log_row

    await_recv(kvx_recv, 2, NX - 1)
    part = kv_send[mx]
    for dx in (1, 2, 3):
        part = part + kvx_recv[(mx + dx) % NX]
    kvz_send[...] = part
    for dz in (4, 3, 5, 2, 6, 1, 7):
        send(kvz_send.at[(mz + dz) % NZ], kvz_recv.at[mz], KVZ, at((dz, 0)))

    for copy in cached:
        copy.wait()
    pos = iota((1, POS), 1) + me * POS
    diag = iota((PROPS, LANES), 1) - iota((PROPS, LANES), 0)
    corner = jnp.where(iota((PROPS, LANES), 0) == 0, iota((PROPS, LANES), 1) - 2 * PROPS, -1)
    for turn in (0, 1, 3, 2):
        s = (s_me + turn) % SEQS
        await_recv(qn_recv, QN + s, HEADS if turn else HEADS - 1)
        base = len_s[s] + acc_s[s]
        live = pos < base
        gates = g_v[s]
        bound = jnp.sum(jnp.where(pos == base - 1, gates, 0.0), axis=1, keepdims=True)
        for t in range(HEADS // 2):
            m0 = qn_recv[s * HEADS + 2 * t].astype(F32)
            m1 = qn_recv[s * HEADS + 2 * t + 1].astype(F32)
            lhs = jnp.concatenate(
                [
                    jnp.where(low8, m0, 0.0),
                    jnp.where(low8, swap(m0), 0.0),
                    jnp.where(low8, 0.0, swap(m1)),
                    jnp.where(low8, 0.0, m1),
                ],
                axis=0,
            ).astype(BF16)
            keys = k_v[s, :, pl.ds(t * LANES, LANES)]
            values = v_v[s, :, pl.ds(t * LANES, LANES)]
            scores = dot(lhs, keys, ((1,), (1,))) * DH**-0.5
            gate_rows = jnp.concatenate(
                [
                    jnp.broadcast_to(gates[2 * t : 2 * t + 1], (PROPS, POS)),
                    jnp.broadcast_to(gates[2 * t + 1 : 2 * t + 2], (PROPS, POS)),
                ],
                axis=0,
            )
            scores = jnp.where(live, scores - gate_rows, MASKED)
            peak = jnp.max(scores, axis=1, keepdims=True)
            weights = jnp.where(live, jnp.exp(scores - peak), 0.0)
            total = jnp.sum(weights, axis=1, keepdims=True)
            part = dot(weights.astype(BF16), values, ((1,), (0,)))
            at_pair = s % 2 * HEADS + 2 * t
            p_send[at_pair, s // 2] = jnp.where(low8, part[:8], swap(part[8:16])).astype(BF16)
            p_send[at_pair + 1, s // 2] = jnp.where(
                low8, swap(part[16:24]), part[24:32]
            ).astype(BF16)
            for odd in range(2):
                rows_at = slice(odd * PROPS, (odd + 1) * PROPS)
                head = 2 * t + odd
                shift = s // 2 * DH
                tile = jnp.where(diag == shift, peak[rows_at], 0.0)
                tile = jnp.where(diag == PROPS + shift, total[rows_at], tile)
                tile = jnp.where(corner == shift, bound[head : head + 1], tile)
                row = jnp.sum(tile, axis=0, keepdims=True)
                if turn in (2, 3):
                    row = row + ps_send[s % 2 * HEADS + head]
                ps_send[s % 2 * HEADS + head] = row
        if turn not in (2, 3):
            continue
        for j in range(HEADS):
            head = (pair + j) % HEADS
            at_pair = s % 2 * HEADS + head
            target = (at_pair // NX + 2) % (NZ // 2) * NX + (head + 1) % NX
            if turn == 3 and j == 0:
                targets = (other_half,)
            else:
                targets = (target, target + HALF)
            for target in targets:
                send(p_send.at[at_pair], p_recv.at[me], PS, target)
                send(ps_send.at[at_pair], ps_recv.at[me], PS + 1, target)
    p_recv[me] = p_send[pair]
    ps_recv[me] = ps_send[pair]

    await_recv(kvz_recv, KVZ, NZ - 1)
    raw_kv = kvz_send[mz]
    for dz in range(1, NZ):
        raw_kv = raw_kv + kvz_recv[(mz + dz) % NZ]
    raw_kv = raw_kv * inverse
    mean_key = jnp.sum(jnp.where(low16, raw_kv * raw_kv, 0.0), axis=1, keepdims=True) / DH
    gain = kg_v[...].reshape(1, DH)
    gain = jnp.concatenate([gain, gain], axis=1)
    kv_new = jnp.where(low16, raw_kv * lax.rsqrt(mean_key + EPSILON) * gain, raw_kv).astype(BF16)
    kvn_send[...] = kv_new
    for owner in range(FIRST_OWNER, N_KV):

        @pl.when(me != owner)
        def _():
            send(kvn_send, kvn_recv.at[me], KVN, owner)

        @pl.when(me == owner)
        def _():
            kvn_recv[me] = kv_new

    q32 = q_packed.astype(F32)
    q_rows = jnp.concatenate(
        [jnp.where(low8, q32, 0.0), jnp.where(low8, swap(q32), 0.0)], axis=0
    ).astype(BF16)
    tree = dot(q_rows, kv_new, ((1,), (1,))) * DH**-0.5 - path_row
    tree_live = ancestors > 0.5
    tree = jnp.where(tree_live, tree, MASKED)
    tree_max = jnp.max(tree, axis=1, keepdims=True)
    tree_weights = jnp.where(tree_live, jnp.exp(tree - tree_max), 0.0)
    tree_total = jnp.sum(tree_weights, axis=1, keepdims=True)
    tree_sum = dot(tree_weights.astype(BF16), kv_new, ((1,), (0,)))
    tree_packed = jnp.where(low8, swap(tree_sum[:8]), tree_sum[8:])
    t_send[...] = tree_packed
    tile = jnp.where(diag == 0, tree_max, 0.0)
    tile = jnp.where(diag == PROPS, tree_total, tile)
    ts_send[...] = jnp.sum(tile, axis=0, keepdims=True)
    for dz in (2, NZ - 2):
        send(t_send, t_buf.at[half], TR, at((dz, 1)))
        send(ts_send, ts_buf.at[half], TR + 1, at((dz, 1)))

    gain = hg_v[...].reshape(1, DH)
    gain = jnp.concatenate([gain, gain], axis=1)
    await_recv(t_buf, TR, 2)
    await_recv(ts_buf, TR + 1, 2)
    await_recv(ps_recv, PS + 1, N_KV - 1)
    await_recv(p_recv, PS, N_KV - 1)
    both_t = ps_recv[...].reshape(N_KV, LANES).T
    for k in range(2):
        stats_t = both_t[k * DH : (k + 1) * DH]
        peaks = stats_t[:PROPS]
        bound = jnp.sum(stats_t[2 * PROPS : 2 * PROPS + 1], axis=1, keepdims=True)
        tree_row = ts_buf[k]
        tree_max = jnp.sum(jnp.where(diag == 0, tree_row, 0.0), axis=1, keepdims=True) - bound
        tree_total = jnp.sum(jnp.where(diag == PROPS, tree_row, 0.0), axis=1, keepdims=True)
        top = jnp.maximum(jnp.max(peaks, axis=1, keepdims=True), tree_max)
        factors = jnp.exp(peaks - top)
        tree_factor = jnp.exp(tree_max - top)
        total = (
            jnp.sum(factors * stats_t[PROPS : 2 * PROPS], axis=1, keepdims=True)
            + tree_total * tree_factor
        )
        acc = [t_buf[k] * jnp.where(low8, tree_factor[:8], tree_factor[8:])] + [None] * 3
        for i in range(N_KV):
            factor = jnp.where(low8, factors[:8, i : i + 1], factors[8:, i : i + 1])
            term = p_recv[i, k].astype(F32) * factor
            acc[i % 4] = term if acc[i % 4] is None else acc[i % 4] + term
        weighted = (acc[0] + acc[1]) + (acc[2] + acc[3])
        attended = weighted / jnp.where(low8, total[:8], total[8:])
        square = attended * attended
        mean_low = jnp.sum(jnp.where(low8, square, 0.0), axis=1, keepdims=True) / DH
        mean_high = jnp.sum(jnp.where(low8, 0.0, square), axis=1, keepdims=True) / DH
        n_send[k] = (
            attended * lax.rsqrt(jnp.where(low8, mean_low, mean_high) + EPSILON) * gain
        ).astype(BF16)

    slot = tp * HALF + pair
    for o in NEAR:
        for core in (tp, 1 - tp):
            if o == (0, 0) and core is tp:
                continue
            send(n_send, n_recv.at[slot], NR, at(o), core, recv=NR + group)
    n_recv[slot] = n_send[...]

    @pl.when(s_me == 0)
    def _():
        await_recv(gl_recv, GL, HEADS - 1)

    @pl.when(s_me != 0)
    def _():
        await_recv(gl_recv, GL, HEADS)

    logs = gl_recv[...].reshape(HEADS, LANES)
    for s in range(SEQS):
        gates_ref[s] = logs[:, s * PROPS : (s + 1) * PROPS]

    @pl.when(me >= FIRST_OWNER)
    def _():
        await_recv(kvn_recv, KVN, N_KV - 1)
        kvn_ref[...] = kvn_recv[...]

    @pl.when(me < FIRST_OWNER)
    def _():
        kvn_ref[...] = jnp.zeros_like(kvn_ref)

    await_recv(wo_v, WO, 1)
    for turn in (0, 2, 1, 3):
        s = (group + turn) % SEQS
        if turn < 2:
            await_recv(n_recv, NR + s % 2, HALF if turn else HALF - 1)
        layer_sum = None
        for core in range(2):
            tiles = []
            for t in range(HEADS // 2):
                spot = core * HALF + s % 2 * HEADS + 2 * t
                m0 = n_recv[spot, s // 2].astype(F32)
                m1 = n_recv[spot + 1, s // 2].astype(F32)
                tiles.append(
                    jnp.concatenate(
                        [jnp.where(low8, m0, swap(m1)), jnp.where(low8, swap(m0), m1)], axis=0
                    ).astype(BF16)
                )
            term = dot(jnp.concatenate(tiles, axis=1), wo_v[core], ((1,), (1,)))
            term = term.astype(BF16).astype(F32)
            layer_sum = term if layer_sum is None else layer_sum + term
        out_ref[s] = layer_sum.astype(BF16)

    await_send(q_send, 0, N_KV - 1)
    await_send(st_recv, 1, N_KV - 1)
    await_send(kvx_recv, 2, NX - 1)
    await_send(kvz_recv, KVZ, NZ - 1)
    await_send(t_buf, TR, 2)
    await_send(ts_buf, TR + 1, 2)
    await_send(qn_recv, QN, N_KV - 1)
    await_send(wo_v, WO, 1)

    @pl.when(s_me == 0)
    def _():
        await_send(st_recv, GL, N_KV - 1)

    @pl.when(me >= FIRST_OWNER)
    def _():
        await_send(kvn_recv, KVN, N_KV - FIRST_OWNER - 1)

    @pl.when(me < FIRST_OWNER)
    def _():
        await_send(kvn_recv, KVN, N_KV - FIRST_OWNER)

    await_send(p_recv, PS, N_KV - 1)
    await_send(ps_recv, PS + 1, N_KV - 1)
    await_send(n_recv, NR, N_KV - 1)


def cache_kernel(
    key_cache,
    value_cache,
    kvn,
    lengths_in,
    accepted_in,
    layer_in,
    gates_in,
    keys_in,
    values_in,
    layer_out,
    new_keys,
    new_values,
    gates_out,
    k_v,
    v_v,
    lengths,
    accepted,
    sem,
    small_sem,
):
    me = lax.axis_index("kv")
    sides = ((key_cache, k_v, new_keys), (value_cache, v_v, new_values))
    ends = [
        pltpu.make_async_copy(layer_in, layer_out, sem.at[0]),
        pltpu.make_async_copy(gates_in, gates_out, sem.at[1]),
    ]
    for copy in ends:
        copy.start()

    def write(s, c, side, patched):
        src, buf, dst = sides[side]
        rows = pl.ds(pl.multiple_of(c * CHUNK, CHUNK), CHUNK)
        return pltpu.make_async_copy(
            (buf if patched else src).at[s, rows], dst.at[s, rows], sem.at[2 + s]
        )

    def whole(s, src, dst):
        return pltpu.make_async_copy(src.at[s], dst.at[s], sem.at[2 + s])

    @pl.when((me >= EARLY) & (me < FIRST_OWNER))
    def _():
        for s in range(SEQS):
            for src, _, dst in sides:
                whole(s, src, dst).start()

    low = iota((CHUNK, LANES), 1) < DH

    @pl.when(me >= FIRST_OWNER)
    def _():
        small = [
            pltpu.make_async_copy(lengths_in, lengths, small_sem.at[0]),
            pltpu.make_async_copy(accepted_in, accepted, small_sem.at[1]),
        ]
        for copy in small:
            copy.start()
        for copy in small:
            copy.wait()
        for s in range(SEQS):
            offset = lengths[s] + accepted[s] - me * POS
            for c in range(POS // CHUNK):
                clear = (offset >= (c + 1) * CHUNK) | (offset + PROPS <= c * CHUNK)

                @pl.when(clear)
                def _():
                    for side in range(2):
                        write(s, c, side, False).start()

        for s in range(SEQS):
            offset = lengths[s] + accepted[s] - me * POS

            def patch(c):
                slot = iota((CHUNK, 1), 0) + c * CHUNK - offset
                hit = (slot >= 0) & (slot < PROPS)
                placing = (slot == iota((CHUNK, PROPS), 1)).astype(BF16)
                rows = pl.ds(pl.multiple_of(c * CHUNK, CHUNK), CHUNK)
                for t in range(HEADS // 2):
                    w0 = dot(placing, kvn[s * HEADS + 2 * t], ((1,), (0,)))
                    w1 = dot(placing, kvn[s * HEADS + 2 * t + 1], ((1,), (0,)))
                    at = (s, rows, pl.ds(t * LANES, LANES))
                    k_v[at] = jnp.where(
                        hit, jnp.where(low, w0, swap(w1)), key_cache[at].astype(F32)
                    ).astype(BF16)
                    v_v[at] = jnp.where(
                        hit, jnp.where(low, swap(w0), w1), value_cache[at].astype(F32)
                    ).astype(BF16)
                for side in range(2):
                    write(s, c, side, True).start()

            first = jnp.maximum(offset, 0) // CHUNK
            last = jnp.minimum(offset + PROPS - 1, POS - 1) // CHUNK

            @pl.when((offset > -PROPS) & (offset < POS))
            def _():
                patch(first)

                @pl.when(last > first)
                def _():
                    patch(last)

    @pl.when(me >= EARLY)
    def _():
        for s in range(SEQS):
            for src, _, dst in sides:
                whole(s, src, dst).wait()

    for copy in ends:
        copy.wait()


def shards(*args):
    hbm = pl.BlockSpec(memory_space=pltpu.HBM)
    vmem = pl.BlockSpec(memory_space=pltpu.VMEM)
    operands = list(args)
    operands[5] = operands[5].T
    operands[10] = operands[10].T
    operands = [pltpu.with_memory_space_constraint(a, pltpu.HBM) for a in operands]
    key_cache, value_cache = args[11], args[12]
    early_keys, early_values, token = pl.pallas_call(
        early_kernel,
        out_shape=(
            jax.ShapeDtypeStruct(key_cache.shape, BF16),
            jax.ShapeDtypeStruct(value_cache.shape, BF16),
            jax.ShapeDtypeStruct((8, LANES), F32),
        ),
        in_specs=[hbm, hbm],
        out_specs=(hbm, hbm, vmem),
        scratch_shapes=[
            pltpu.VMEM((SEQS, POS, WIDTH), BF16),
            pltpu.VMEM((SEQS, POS, WIDTH), BF16),
            pltpu.SemaphoreType.DMA((2 * SEQS,)),
            pltpu.SemaphoreType.DMA((2 * SEQS,)),
        ],
        compiler_params=pltpu.CompilerParams(vmem_limit_bytes=16 * 2**20),
        name="early",
    )(operands[11], operands[12])
    layer_out, gates, kvn = pl.pallas_call(
        layer_kernel,
        out_shape=(
            jax.ShapeDtypeStruct((SEQS, PROPS, FEATS), BF16),
            jax.ShapeDtypeStruct((SEQS, HEADS, PROPS), F32),
            jax.ShapeDtypeStruct((N_KV, PROPS, LANES), BF16),
        ),
        in_specs=[hbm] * len(operands) + [pl.BlockSpec(memory_space=pl.ANY)],
        out_specs=(vmem, vmem, vmem),
        scratch_shapes=[
            pltpu.VMEM((SEQS, PROPS, FEATS), BF16),
            pltpu.VMEM((FEATS, 3 * WIDTH), BF16),
            pltpu.VMEM((2 * HEADS, LANES), BF16),
            pltpu.VMEM((2, FEATS, WIDTH), BF16),
            pltpu.VMEM((FEATS,), F32),
            pltpu.VMEM((DH,), F32),
            pltpu.VMEM((DH,), F32),
            pltpu.VMEM((DH,), F32),
            pltpu.VMEM((SEQS, PROPS), jnp.int32),
            pltpu.SMEM((2 * HEADS,), F32),
            pltpu.SMEM((SEQS,), jnp.int32),
            pltpu.SMEM((SEQS,), jnp.int32),
            pltpu.VMEM((SEQS, POS, WIDTH), BF16),
            pltpu.VMEM((SEQS, POS, WIDTH), BF16),
            pltpu.VMEM((SEQS, HEADS, POS), F32),
            pltpu.VMEM((N_KV, 8, LANES), F32),
            pltpu.VMEM((N_KV, 8, LANES), F32),
            pltpu.VMEM((2 * HEADS, 1, LANES), F32),
            pltpu.VMEM((N_KV, 1, LANES), F32),
            pltpu.VMEM((NX, NZ, PROPS, LANES), F32),
            pltpu.VMEM((NX, NZ, PROPS, LANES), F32),
            pltpu.VMEM((NZ, PROPS, LANES), F32),
            pltpu.VMEM((NZ, PROPS, LANES), F32),
            pltpu.VMEM((8, LANES), BF16),
            pltpu.VMEM((N_KV, 8, LANES), BF16),
            pltpu.VMEM((PROPS, LANES), BF16),
            pltpu.VMEM((N_KV, PROPS, LANES), BF16),
            pltpu.VMEM((1, LANES), F32),
            pltpu.VMEM((HEADS, 1, LANES), F32),
            pltpu.VMEM((HALF, 2, 8, LANES), BF16),
            pltpu.VMEM((N_KV, 2, 8, LANES), BF16),
            pltpu.VMEM((HALF, 1, LANES), F32),
            pltpu.VMEM((N_KV, 1, LANES), F32),
            pltpu.VMEM((2, 8, LANES), F32),
            pltpu.VMEM((2, 1, LANES), F32),
            pltpu.VMEM((2, 8, LANES), BF16),
            pltpu.VMEM((2 * HALF, 2, 8, LANES), BF16),
            pltpu.VMEM((8, LANES), F32),
            pltpu.VMEM((1, LANES), F32),
            pltpu.SemaphoreType.DMA((20,)),
            pltpu.SemaphoreType.DMA((24,)),
            pltpu.SemaphoreType.DMA((24,)),
        ],
        compiler_params=pltpu.CompilerParams(
            collective_id=0, has_side_effects=True, vmem_limit_bytes=24 * 2**20
        ),
        name="layer",
    )(*operands, token)
    layer_out, new_keys, new_values, gates = pl.pallas_call(
        cache_kernel,
        out_shape=(
            jax.ShapeDtypeStruct(layer_out.shape, BF16),
            jax.ShapeDtypeStruct(key_cache.shape, BF16),
            jax.ShapeDtypeStruct(value_cache.shape, BF16),
            jax.ShapeDtypeStruct(gates.shape, F32),
        ),
        in_specs=[vmem, vmem, vmem, hbm, hbm, vmem, vmem, hbm, hbm],
        out_specs=(hbm, hbm, hbm, hbm),
        input_output_aliases={7: 1, 8: 2},
        scratch_shapes=[
            pltpu.VMEM((SEQS, POS, WIDTH), BF16),
            pltpu.VMEM((SEQS, POS, WIDTH), BF16),
            pltpu.SMEM((SEQS,), jnp.int32),
            pltpu.SMEM((SEQS,), jnp.int32),
            pltpu.SemaphoreType.DMA((2 + SEQS,)),
            pltpu.SemaphoreType.DMA((2,)),
        ],
        compiler_params=pltpu.CompilerParams(vmem_limit_bytes=16 * 2**20),
        name="cache",
    )(
        key_cache,
        value_cache,
        kvn,
        operands[14],
        operands[15],
        layer_out,
        gates,
        early_keys,
        early_values,
    )
    return layer_out, new_keys, new_values, jnp.transpose(gates, (0, 2, 1))


def solution(mesh):
    placed = (
        P("dp", None, "kv"),
        P("kv"),
        P("kv", "tp"),
        P("kv", "tp"),
        P("kv", "tp"),
        P(),
        P(),
        P(),
        P(),
        P(),
        P("tp", "kv"),
        P("dp", "kv", "tp"),
        P("dp", "kv", "tp"),
        P("dp", "tp", "kv"),
        P("dp"),
        P("dp"),
        P("dp", None),
    )
    return jax.shard_map(
        shards,
        mesh=mesh,
        in_specs=placed,
        out_specs=(
            P("dp", None, "kv"),
            P("dp", "kv", "tp"),
            P("dp", "kv", "tp"),
            P("dp", None, "tp"),
        ),
        check_vma=False,
    )
```
